128 devices in a mesh: sp: 16 (over z, x), fs: 4 (over y), tp: 2 (over core).
Axes of the slice: x: 4, y: 4, z: 4, core: 2. Of those that a mesh axis runs over, the one named last changes fastest.
Arguments:
- tokens: bfloat16 [49152, 2048], P(('fs', 'sp'), 'tp'), parts along dimension 0, may hold values from -6 to 6
- norm_gain: bfloat16 [2048], replicated, may hold values from 0.099609375 to 1.8984375
- w_query: bfloat16 [2048, 1024], P(None, 'tp'), may hold values from -0.125 to 0.125
- w_key: bfloat16 [2048, 1024], P(None, 'tp'), may hold values from -0.125 to 0.125
- w_value: bfloat16 [2048, 1024], P(None, 'tp'), may hold values from -0.125 to 0.125
- log_decay: float32 [8, 12288], P('tp', 'sp'), may hold values from -1 to 0
- w_conv_in: bfloat16 [2048, 1024], P(None, 'tp'), may hold values from -0.125 to 0.125
- w_conv_pre: bfloat16 [2048, 1024], P(None, 'tp'), may hold values from -0.125 to 0.125
- w_conv_post: bfloat16 [2048, 1024], P(None, 'tp'), may hold values from -0.125 to 0.125
- conv_taps: bfloat16 [3, 1024], P(None, 'tp'), may hold values from -3 to 3
- w_out_ret: bfloat16 [1024, 2048], replicated, may hold values from -0.125 to 0.125
- w_out_conv: bfloat16 [1024, 2048], replicated, may hold values from -0.125 to 0.125
Outputs:
- mixed: bfloat16 [49152, 2048], P(('fs', 'sp', 'tp')), parts along dimension 0
The draws below stay inside these ranges and needn't reach their ends.
There are 4 independent parts, one for each index of `fs`. The reference program is written for one: setup_inputs(seed, part) draws one part's arguments, and reference() takes and returns one part's arrays. A program takes and returns all parts, laid end to end along the dimension named above; an argument that names none is the same for every part. Nothing has to cross between parts.
All inputs are finite; a program needn't handle non-finite values.
Results may differ from the reference program's by a relative error of at most 0.012.
Values may be sent and summed in bfloat16 or wider, within the bound.
A program may use at most 128 MiB of HBM per device.

```python
import math
import jax
import jax.numpy as jnp
from jax import lax

D = 2048
RETENTION_HEADS = 8
DH = 128
CW = 1024
TAPS = 3
SPAN = 128
TOK_DEV = 768
SEQUENCE_LENGTH = 12288
RW = 1024


def draw_log_decay(key, part):
    head_order = jax.random.permutation(jax.random.fold_in(key, 1), RETENTION_HEADS)
    fast_heads = head_order < RETENTION_HEADS // 2
    token_position = jnp.arange(SEQUENCE_LENGTH, dtype=jnp.int32)
    segment = token_position // TOK_DEV
    jitter = jax.random.uniform(jax.random.fold_in(key, 2), (SEQUENCE_LENGTH // TOK_DEV,), jnp.float32)
    factor = 2.0 ** (1.5 * (segment % 2).astype(jnp.float32) + 0.5 * jitter[segment])
    slow_scale = jax.random.uniform(jax.random.fold_in(key, 3), (RETENTION_HEADS,), jnp.float32, 0.03, 0.09)
    span_length = jax.random.uniform(jax.random.fold_in(key, 4), (RETENTION_HEADS,), jnp.float32, 50.0, 80.0)
    ln_ten = math.log(10.0)
    fast_rate = ln_ten / span_length[:, None] * factor[None, :] * 0.5
    slow_rate = ln_ten * slow_scale[:, None] * factor[None, :] / SEQUENCE_LENGTH
    decay_speed = jnp.where(fast_heads[:, None], fast_rate, slow_rate)
    spike_position = jax.random.randint(jax.random.fold_in(key, 5), (2,), 0, SEQUENCE_LENGTH)
    spike_penalty = jax.random.uniform(jax.random.fold_in(key, 6), (RETENTION_HEADS, 2), jnp.float32, 0.2, 0.4)
    spike_events = jnp.where(token_position[None, :] == spike_position[0], jnp.log1p(-spike_penalty[:, 0:1]), 0.0)
    spike_events = spike_events + jnp.where(token_position[None, :] == spike_position[1], jnp.log1p(-spike_penalty[:, 1:2]), 0.0)
    return (spike_events - decay_speed).astype(jnp.float32)


def steps_of(stream_key, shape, shards, low, largest):
    loudness = 1.0
    for position, shards_of in shards:
        draws = jax.random.uniform(jax.random.fold_in(jax.random.fold_in(stream_key, 6), position), (shards_of,), jnp.float32, low / len(shards), largest / len(shards))
        loudness = loudness * jnp.repeat(jnp.exp(draws), shape[position] // shards_of).reshape((-1,) + (1,) * (len(shape) - 1 - position))
    return loudness


def normal_values(rng, shape, deviation, bound, cuts=(), kind=jnp.bfloat16):
    gain = steps_of(rng, shape, cuts, -0.22, 0.18) if cuts else 1.0
    result = jax.random.normal(rng, shape, jnp.float32) * deviation * gain
    return jnp.minimum(jnp.maximum(result, -bound), bound).astype(kind)


def setup_inputs(seed: int = 0, part: int = 0) -> dict:
    splits = jax.random.split(jax.random.key(seed), 13)
    own_keys = jax.random.split(jax.random.fold_in(splits[12], part), 13)
    return {
        "tokens": normal_values(own_keys[0], (SEQUENCE_LENGTH, D), 1.0, 6.0, ((0, 16), (1, 2))),
        "norm_gain": jnp.clip(1.0 + 0.18 * jax.random.normal(splits[1], (D,), jnp.float32), 0.099609375, 1.8984375).astype(jnp.bfloat16),
        "w_query": normal_values(splits[2], (D, RW), D ** -0.5, 0.125, ((1, 2),)),
        "w_key": normal_values(splits[3], (D, RW), D ** -0.5, 0.125, ((1, 2),)),
        "w_value": normal_values(splits[4], (D, RW), D ** -0.5, 0.125, ((1, 2),)),
        "log_decay": draw_log_decay(jax.random.fold_in(splits[12], 71), part),
        "w_conv_in": normal_values(splits[6], (D, CW), D ** -0.5, 0.125, ((1, 2),)),
        "w_conv_pre": normal_values(splits[7], (D, CW), D ** -0.5, 0.125, ((1, 2),)),
        "w_conv_post": normal_values(splits[8], (D, CW), D ** -0.5, 0.125, ((1, 2),)),
        "conv_taps": normal_values(splits[9], (TAPS, CW), 0.577, 3.0, ((1, 2),)),
        "w_out_ret": normal_values(splits[10], (RW, D), (RW + CW) ** -0.5, 0.125),
        "w_out_conv": normal_values(splits[11], (CW, D), (RW + CW) ** -0.5, 0.125),
    }


epsilon = 1e-06

def rotate(vectors, positions):
    halfway = vectors.shape[-1] // 2
    inverse = 10000.0 ** (-jnp.arange(halfway, dtype=jnp.float32) / halfway)
    angles = positions.astype(jnp.float32)[:, None] * inverse[None, :]
    cosines = jnp.cos(angles)[:, None, :]
    sinusoid = jnp.sin(angles)[:, None, :]
    leading = vectors[..., :halfway]
    trailing = vectors[..., halfway:]
    return jnp.concatenate([leading * cosines - trailing * sinusoid, leading * sinusoid + trailing * cosines], axis=-1)

def retain(queries, keys, values, log_decay):
    blocks = SEQUENCE_LENGTH // SPAN
    query_blocks = queries.reshape(blocks, SPAN, RETENTION_HEADS, DH)
    key_blocks = keys.reshape(blocks, SPAN, RETENTION_HEADS, DH)
    value_blocks = values.reshape(blocks, SPAN, RETENTION_HEADS, DH)
    decay_blocks = log_decay.reshape(RETENTION_HEADS, blocks, SPAN).transpose(1, 0, 2)
    lower_mask = jnp.tril(jnp.ones((SPAN, SPAN), bool))

    def advance(carried, inputs):
        query_block, key_block, value_block, decay_block = inputs
        cumulative = jnp.cumsum(decay_block, axis=-1)
        differences = cumulative[:, :, None] - cumulative[:, None, :]
        decay_weights = jnp.where(lower_mask[None], jnp.exp(jnp.minimum(differences, 0.0)), 0.0)
        query_float = query_block.astype(jnp.float32)
        key_float = key_block.astype(jnp.float32)
        value_float = value_block.astype(jnp.float32)
        scores = jnp.einsum('shd,thd->hst', query_float, key_float)
        mix_weights = lax.optimization_barrier((scores * decay_weights).astype(jnp.bfloat16)).astype(jnp.float32)
        inside = jnp.einsum('hst,thd->shd', mix_weights, value_float)
        across = jnp.einsum('shd,hde->she', query_float, carried, precision=lax.Precision.HIGHEST)
        retained = inside + jnp.exp(cumulative).T[:, :, None] * across
        last_decay = cumulative[:, -1]
        tail_decay = jnp.exp(last_decay[:, None] - cumulative)
        fresh_state = jnp.einsum('shd,she->hde', key_float, value_float * tail_decay.T[:, :, None], precision=lax.Precision.HIGHEST)
        return (jnp.exp(last_decay)[:, None, None] * carried + fresh_state, retained)
    initial = jnp.zeros((RETENTION_HEADS, DH, DH), jnp.float32)
    unused_state, retained = lax.scan(advance, initial, (query_blocks, key_blocks, value_blocks, decay_blocks))
    retained = retained.reshape(SEQUENCE_LENGTH, RETENTION_HEADS, DH)
    normalized = retained * lax.rsqrt(lax.optimization_barrier(jnp.mean(retained * retained, axis=-1, keepdims=True)) + epsilon)
    return normalized.astype(jnp.bfloat16).reshape(SEQUENCE_LENGTH, RETENTION_HEADS * DH)

def reference(tokens, norm_gain, w_query, w_key, w_value, log_decay, w_conv_in, w_conv_pre, w_conv_post, conv_taps, w_out_ret, w_out_conv):
    floats = tokens.astype(jnp.float32)
    normed = (floats * lax.rsqrt(lax.optimization_barrier(jnp.mean(floats * floats, axis=-1, keepdims=True)) + epsilon) * norm_gain.astype(jnp.float32)).astype(jnp.bfloat16)
    positions = jnp.arange(SEQUENCE_LENGTH, dtype=jnp.int32)

    def project(weight):
        return jnp.dot(normed, weight, preferred_element_type=jnp.float32)
    queries = rotate(project(w_query).reshape(SEQUENCE_LENGTH, RETENTION_HEADS, DH), positions).astype(jnp.bfloat16)
    keys = (rotate(project(w_key).reshape(SEQUENCE_LENGTH, RETENTION_HEADS, DH), positions) * DH ** (-0.5)).astype(jnp.bfloat16)
    values = project(w_value).astype(jnp.bfloat16).reshape(SEQUENCE_LENGTH, RETENTION_HEADS, DH)
    ret_out = retain(queries, keys, values, log_decay)
    conv_in = lax.optimization_barrier(project(w_conv_in).astype(jnp.bfloat16))
    conv_pre = lax.optimization_barrier(project(w_conv_pre).astype(jnp.bfloat16))
    conv_post = lax.optimization_barrier(project(w_conv_post).astype(jnp.bfloat16))
    gated_in = (conv_pre.astype(jnp.float32) * conv_in.astype(jnp.float32)).astype(jnp.bfloat16)
    padded = jnp.pad(gated_in, ((TAPS - 1, 0), (0, 0)))
    convolved = jnp.zeros((SEQUENCE_LENGTH, CW), jnp.float32)
    for tap_index in range(TAPS):
        convolved = convolved + conv_taps[tap_index].astype(jnp.float32) * padded[tap_index:tap_index + SEQUENCE_LENGTH].astype(jnp.float32)
    conv_out = (conv_post.astype(jnp.float32) * convolved).astype(jnp.bfloat16)
    mixed_rows = jnp.dot(ret_out, w_out_ret, preferred_element_type=jnp.float32) + jnp.dot(conv_out, w_out_conv, preferred_element_type=jnp.float32)
    return mixed_rows.astype(jnp.bfloat16)
```

```python
import functools

import jax
import jax.numpy as jnp
import numpy as np
from jax import lax
from jax.experimental import pallas as pl
from jax.experimental.pallas import tpu as pltpu
from jax.sharding import PartitionSpec as P

DH = 128
SPAN = 128
ROWS = 768
HALF = 384
BLOCKS = 6
HEADS = 4
KW = 1024
NW = 512
D = 2048
EPS = 1e-06
KEY_SCALE = 128.0 ** -0.5
F32 = jnp.float32
BF16 = jnp.bfloat16
MESH = pl.DeviceIdType.MESH
WEIGHTS = ("wk", "wv", "wq", "wci", "wcp", "wcq")


def rotation_tables(places):
    half = DH // 2
    rate = 10000.0 ** (-np.arange(half, dtype=np.float64) / half)
    inner = np.arange(SPAN, dtype=np.float64)[:, None] * rate[None, :]
    inner = np.concatenate([inner, inner], axis=1)
    sign = np.concatenate([-np.ones(half), np.ones(half)])[None, :]
    within = np.stack(
        [np.cos(inner), np.sin(inner), sign * np.cos(inner), sign * np.sin(inner)]
    ).astype(np.float32)
    start = np.arange(places * BLOCKS, dtype=np.float64) * SPAN
    outer = start[:, None] * rate[None, :]
    outer = np.concatenate([outer, outer], axis=1).reshape(places, BLOCKS, DH)
    bases = np.zeros((places, 16, DH), np.float32)
    bases[:, :BLOCKS] = np.cos(outer)
    bases[:, 8 : 8 + BLOCKS] = np.sin(outer)
    return within, bases


def mm(a, b):
    return jnp.dot(a, b, preferred_element_type=F32)


def kernel(
    tok, gain, ld, taps, wk, wv, wq, wci, wcp, wcq, woc, wor, tabs, bases,
    out,
    xo, go, gp, wbuf, wob, acc, kb, vb, qb, cib, postb, gbuf, cob, cor,
    retb, retr, inside, states, starts, oacc, ssb, pack, pack_far, rot_c, rot_s,
    tabv, basev, gainv, ldv, tapv, ldp, cumr, colrep, lrow, lcol,
    a1, a2, b1, b2, bm, pre,
    sem_tok, sem_small, sem_w, sem_wo,
    ts, tr, l1s, l1r, l2s, l2r, a1s, a1r, a2s, a2r, b1s, b1r, b2s, b2r,
    hs, hr, cs, cr, rs, rr, ps, pr,
):
    sp = lax.axis_index("sp")
    tp = lax.axis_index("tp")
    x = lax.rem(sp, 4)
    z = lax.div(sp, 4)
    other = 1 - tp
    row_peer = [z * 4 + lax.rem(x + k, 4) for k in (1, 2, 3)]
    col_peer = [lax.rem(z + k, 4) * 4 + x for k in (1, 2, 3)]
    after = lax.rem(sp + 1, 16)
    before = lax.rem(sp + 15, 16)

    barrier = pltpu.get_barrier_semaphore()
    pl.semaphore_signal(barrier, inc=1, device_id={"tp": other}, device_id_type=MESH)
    for peer in row_peer + col_peer + [after, before]:
        pl.semaphore_signal(barrier, inc=1, device_id={"sp": peer}, device_id_type=MESH)

    def remote(src, dst, send, recv, where):
        return pltpu.make_async_remote_copy(
            src_ref=src, dst_ref=dst, send_sem=send, recv_sem=recv,
            device_id=where, device_id_type=MESH,
        )

    own_k = pl.multiple_of(tp * KW, KW)
    far_k = pl.multiple_of(other * KW, KW)
    own_n = pl.multiple_of(tp * NW, NW)
    far_n = pl.multiple_of(other * NW, NW)
    own_rows = pl.ds(pl.multiple_of(tp * HALF, HALF), HALF)
    far_rows = pl.ds(pl.multiple_of(other * HALF, HALF), HALF)

    tok_load = [
        pltpu.make_async_copy(
            tok.at[pl.ds(c * 256, 256), :], xo.at[pl.ds(c * 256, 256), :], sem_tok.at[c]
        )
        for c in range(3)
    ]
    small = [
        pltpu.make_async_copy(ld, ldv, sem_small.at[0]),
        pltpu.make_async_copy(gain, gainv, sem_small.at[1]),
        pltpu.make_async_copy(taps, tapv, sem_small.at[2]),
        pltpu.make_async_copy(tabs, tabv, sem_small.at[3]),
        pltpu.make_async_copy(bases.at[sp], basev, sem_small.at[4]),
    ]
    hbm = dict(zip(WEIGHTS, (wk, wv, wq, wci, wcp, wcq)))
    index = {name: i for i, name in enumerate(WEIGHTS)}

    def w_load(name, part):
        i = index[name]
        rows = pl.ds(own_k if part == 0 else far_k, KW)
        return pltpu.make_async_copy(
            hbm[name].at[rows, :], wbuf.at[i, part], sem_w.at[i * 2 + part]
        )

    def wo_load(i, part):
        rows = pl.ds(own_n if part == 0 else far_n, NW)
        return pltpu.make_async_copy(
            (woc, wor)[i].at[rows, :], wob.at[i, part], sem_wo.at[i * 2 + part]
        )

    small[0].start()
    small[1].start()
    for copy in tok_load:
        copy.start()
    w_load("wk", 0).start()
    w_load("wv", 0).start()
    small[4].start()
    small[3].start()
    small[2].start()

    ldp[...] = jnp.zeros_like(ldp)
    small[0].wait()
    for b in range(BLOCKS):
        ldp[b * 8 : b * 8 + HEADS, :] = ldv[:, b * SPAN : (b + 1) * SPAN]
    upper = (
        lax.broadcasted_iota(jnp.int32, (SPAN, SPAN), 0)
        <= lax.broadcasted_iota(jnp.int32, (SPAN, SPAN), 1)
    )
    ones = jnp.where(upper, 1.0, 0.0).astype(BF16)
    rest = ldp[...]
    total = jnp.zeros((SPAN, SPAN), F32)
    for _ in range(3):
        piece = rest.astype(BF16)
        total = total + mm(piece, ones)
        rest = rest - piece.astype(F32)
    cumr[...] = total
    columns = total.T
    for b in range(BLOCKS):
        for h in range(HEADS):
            i = b * 8 + h
            colrep[b, h] = jnp.broadcast_to(columns[:, i : i + 1], (SPAN, SPAN))

    def block_end(b, h):
        return colrep[b, h, SPAN - 1 : SPAN, :]

    lrow[x] = jnp.zeros((8, SPAN), F32)
    for h in range(HEADS):
        whole = block_end(0, h)
        for b in range(1, BLOCKS):
            whole = whole + block_end(b, h)
        lrow[x, h : h + 1, :] = whole

    lane = lax.broadcasted_iota(jnp.int32, (SPAN, SPAN), 1)
    packed = jnp.zeros((SPAN, SPAN), F32)
    for i in range(BLOCKS):
        if i % 2 == 0:
            tok_load[i // 2].wait()
        rows = slice(i * 128, i * 128 + 128)
        value = xo[rows, :].astype(F32)
        squares = jnp.sum(value * value, axis=1, keepdims=True)
        spread = jnp.broadcast_to(squares, (SPAN, SPAN))
        ssb[rows, :] = spread
        packed = jnp.where(lane == i, spread, packed)
    pack[...] = packed

    pl.semaphore_wait(barrier, 9)
    pack_send = remote(pack, pack_far, ps, pr, {"tp": other})
    pack_send.start()
    l1_send = [
        remote(lrow.at[x], lrow.at[x], l1s.at[k], l1r.at[k], {"sp": row_peer[k]})
        for k in range(3)
    ]
    for copy in l1_send:
        copy.start()
    w_load("wq", 0).start()
    w_load("wci", 0).start()

    small[1].wait()
    small[3].wait()
    small[4].wait()

    def tables(b, carry):
        rows = pl.ds(pl.multiple_of(b * 128, 128), 128)
        base_c = basev[pl.ds(b, 1), :]
        base_s = basev[pl.ds(b + 8, 1), :]
        rot_c[rows, :] = base_c * tabv[0] - base_s * tabv[1]
        rot_s[rows, :] = base_s * tabv[2] + base_c * tabv[3]
        return carry

    lax.fori_loop(0, BLOCKS, tables, 0)
    weight = gainv[:, pl.ds(own_k, KW)].astype(F32)
    pack_send.wait_recv()
    tok_send = [
        remote(
            go.at[pl.ds(c * 256, 256), :], gp.at[pl.ds(c * 256, 256), :],
            ts.at[c], tr.at[c], {"tp": other},
        )
        for c in range(3)
    ]
    for i in range(BLOCKS):
        rows = slice(i * 128, i * 128 + 128)
        level = ssb[rows, :] + jnp.broadcast_to(pack_far[:, i : i + 1], (SPAN, SPAN))
        scale = lax.rsqrt(level * (1.0 / D) + EPS)
        for c in range(KW // 128):
            at = slice(c * 128, c * 128 + 128)
            go[rows, at] = (xo[rows, at].astype(F32) * scale * weight[:, at]).astype(BF16)
        if i in (2, 4):
            tok_send[i // 2 - 1].start()
    tok_send[2].start()

    def near_product(name):
        i = index[name]
        w_load(name, 0).wait()

        def step(n, carry):
            cols = pl.ds(pl.multiple_of(n * 256, 256), 256)
            acc[i, :, cols] = mm(go[...], wbuf[i, 0, :, cols])
            return carry

        lax.fori_loop(0, 2, step, 0)

    near_product("wk")
    w_load("wk", 1).start()
    w_load("wv", 1).start()
    near_product("wv")
    w_load("wq", 1).start()
    w_load("wci", 1).start()
    near_product("wq")
    w_load("wcp", 0).start()
    w_load("wcp", 1).start()
    near_product("wci")
    w_load("wcq", 0).start()
    w_load("wcq", 1).start()

    for copy in l1_send:
        copy.wait_recv()
    line = [lrow[i] for i in range(4)]

    def between(low, high):
        parts = [
            jnp.where(jnp.logical_and(i > low, i < high), line[i], 0.0) for i in range(4)
        ]
        return (parts[0] + parts[1]) + (parts[2] + parts[3])

    row_total = (line[0] + line[1]) + (line[2] + line[3])
    lcol[z, 0] = row_total
    lcol[z, 1] = between(x, 4)
    l2_send = [
        remote(lcol.at[z], lcol.at[z], l2s.at[k], l2r.at[k], {"sp": col_peer[k]})
        for k in range(3)
    ]
    for copy in l2_send:
        copy.start()

    for copy in tok_send:
        copy.wait_recv()

    def rotated(value):
        return value * rot_c[...] + pltpu.roll(value, 64, axis=1) * rot_s[...]

    exchange = []
    for n in range(2):
        cols = slice(n * 256, n * 256 + 256)
        if n == 0:
            w_load("wk", 1).wait()
        kk = acc[0, :, cols] + mm(gp[...], wbuf[0, 1, :, cols])
        for j in range(2):
            at = slice(n * 256 + j * 128, n * 256 + j * 128 + 128)
            kb[:, at] = (rotated(kk[:, j * 128 : j * 128 + 128]) * KEY_SCALE).astype(BF16)
        if n == 0:
            w_load("wv", 1).wait()
        vv = acc[1, :, cols] + mm(gp[...], wbuf[1, 1, :, cols])
        for j in range(2):
            at = slice(n * 256 + j * 128, n * 256 + j * 128 + 128)
            vb[:, at] = vv[:, j * 128 : j * 128 + 128].astype(BF16)
        slot = a1.at[x] if n == 0 else b1.at[z]
        for j in range(2):
            h = n * 2 + j
            at = slice(h * 128, h * 128 + 128)
            whole = None
            for b in range(BLOCKS):
                rows = slice(b * 128, b * 128 + 128)
                end = block_end(b, h)
                tail = jnp.exp(end - colrep[b, h])
                weighted = (vb[rows, at].astype(F32) * tail).astype(BF16)
                fresh = lax.dot_general(
                    kb[rows, at], weighted, (((0,), (0,)), ((), ())),
                    preferred_element_type=F32,
                )
                states[b, h] = fresh
                whole = fresh if whole is None else jnp.exp(end) * whole + fresh
            slot[j] = whole.astype(BF16)
        for k in range(3):
            if n == 0:
                copy = remote(a1.at[x], a1.at[x], a1s.at[k], a1r.at[k], {"sp": row_peer[k]})
            else:
                copy = remote(b1.at[z], b1.at[z], b1s.at[k], b1r.at[k], {"sp": col_peer[k]})
            copy.start()
            exchange.append(copy)

    w_load("wq", 1).wait()

    def query_step(n, carry):
        cols = pl.ds(pl.multiple_of(n * 256, 256), 256)
        qq = acc[2, :, cols] + mm(gp[...], wbuf[2, 1, :, cols])
        for j in range(2):
            at = pl.ds(pl.multiple_of(n * 256 + j * 128, 128), 128)
            qb[:, at] = rotated(qq[:, j * 128 : j * 128 + 128]).astype(BF16)
        return carry

    lax.fori_loop(0, 2, query_step, 0)

    w_load("wci", 1).wait()

    def conv_in_step(n, carry):
        cols = pl.ds(pl.multiple_of(n * 256, 256), 256)
        value = acc[3, :, cols] + mm(gp[...], wbuf[3, 1, :, cols])
        cib[:, cols] = value.astype(BF16)
        return carry

    lax.fori_loop(0, 2, conv_in_step, 0)

    w_load("wcp", 0).wait()
    w_load("wcp", 1).wait()
    for i in range(2):
        for part in range(2):
            wo_load(i, part).start()

    def conv_pre_step(n, carry):
        cols = pl.ds(pl.multiple_of(n * 256, 256), 256)
        value = mm(go[...], wbuf[4, 0, :, cols]) + mm(gp[...], wbuf[4, 1, :, cols])
        pre_gate = value.astype(BF16).astype(F32)
        gated = (pre_gate * cib[:, cols].astype(F32)).astype(BF16).astype(F32)
        for j in range(2):
            gbuf[n * 2 + j, 8 : 8 + ROWS, :] = gated[:, j * 128 : j * 128 + 128]
        return carry

    lax.fori_loop(0, 2, conv_pre_step, 0)
    halo = remote(
        gbuf.at[:, pl.ds(ROWS, 8), :], gbuf.at[:, pl.ds(0, 8), :], hs, hr, {"sp": after}
    )
    halo.start()

    for copy in l2_send:
        copy.wait_recv()
    row_sums = [lcol[i, 0] for i in range(4)]
    suffix = [lcol[i, 1] for i in range(4)]
    before_me = between(-1, x)

    def rows_between(low):
        parts = [
            jnp.where(jnp.logical_and(i > low, i < z), row_sums[i], 0.0) for i in range(4)
        ]
        return (parts[0] + parts[1]) + (parts[2] + parts[3])

    def lane_row(weight, h):
        return weight[h : h + 1, :]

    to_end = [jnp.exp(between(i, 4)) for i in range(4)]
    to_me = [jnp.where(i < x, jnp.exp(between(i, x)), 0.0) for i in range(4)]
    for k in range(3):
        exchange[k].wait_recv()
    for j in range(2):
        parts = [a1[i, j].astype(F32) for i in range(4)]
        row_state = lane_row(to_end[0], j) * parts[0]
        prefix = lane_row(to_me[0], j) * parts[0]
        for i in range(1, 4):
            row_state = row_state + lane_row(to_end[i], j) * parts[i]
            prefix = prefix + lane_row(to_me[i], j) * parts[i]
        pre[j] = prefix
        a2[z, j] = row_state.astype(BF16)
    second = []
    for k in range(3):
        copy = remote(a2.at[z], a2.at[z], a2s.at[k], a2r.at[k], {"sp": col_peer[k]})
        copy.start()
        second.append(copy)
    above = [
        jnp.where(i < z, jnp.exp(suffix[i] + rows_between(i)), 0.0) for i in range(4)
    ]
    for k in range(3):
        exchange[3 + k].wait_recv()
    e_own = jnp.exp(before_me)
    for j in range(2):
        h = 2 + j
        column = lane_row(above[0], h) * b1[0, j].astype(F32)
        for i in range(1, 4):
            column = column + lane_row(above[i], h) * b1[i, j].astype(F32)
        mine = b1[z, j].astype(F32)
        b2[x, j] = (lane_row(e_own, h) * column).astype(BF16)
        for k in range(3):
            target = lax.rem(x + k + 1, 4)
            e_col = jnp.exp(between(-1, target))
            e_mine = jnp.where(x < target, jnp.exp(between(x, target)), 0.0)
            bm[k, j] = (lane_row(e_col, h) * column + lane_row(e_mine, h) * mine).astype(BF16)
    for k in range(3):
        copy = remote(bm.at[k], b2.at[x], b2s.at[k], b2r.at[k], {"sp": row_peer[k]})
        copy.start()
        second.append(copy)

    w_load("wcq", 0).wait()
    w_load("wcq", 1).wait()

    def conv_post_step(n, carry):
        cols = pl.ds(pl.multiple_of(n * 256, 256), 256)
        value = mm(go[...], wbuf[5, 0, :, cols]) + mm(gp[...], wbuf[5, 1, :, cols])
        postb[:, cols] = value.astype(BF16)
        return carry

    lax.fori_loop(0, 2, conv_post_step, 0)

    small[2].wait()
    halo.wait_recv()

    @pl.when(sp == 0)
    def _():
        gbuf[:, 0:8, :] = jnp.zeros((4, 8, 128), F32)

    for c in range(4):
        at = slice(c * 128, c * 128 + 128)
        summed = jnp.zeros((ROWS, 128), F32)
        for i in range(3):
            summed = summed + tapv[i : i + 1, at].astype(F32) * gbuf[c, 6 + i : 6 + i + ROWS, :]
        cob[:, at] = (postb[:, at].astype(F32) * summed).astype(BF16)
    conv_send = remote(cob.at[far_rows, :], cor, cs, cr, {"tp": other})
    conv_send.start()

    lower = (
        lax.broadcasted_iota(jnp.int32, (SPAN, SPAN), 0)
        >= lax.broadcasted_iota(jnp.int32, (SPAN, SPAN), 1)
    )

    def inside_step(b, carry):
        rows = pl.ds(pl.multiple_of(b * 128, 128), 128)
        for h in range(HEADS):
            at = slice(h * 128, h * 128 + 128)
            gap = colrep[b, h] - cumr[pl.ds(b * 8 + h, 1), :]
            weight = jnp.where(lower, jnp.exp(jnp.minimum(gap, 0.0)), 0.0)
            scores = lax.dot_general(
                qb[rows, at], kb[rows, at], (((1,), (1,)), ((), ())),
                preferred_element_type=F32,
            )
            mixed = (scores * weight).astype(BF16)
            inside[rows, at] = mm(mixed, vb[rows, at])
        return carry

    lax.fori_loop(0, BLOCKS, inside_step, 0)

    conv_send.wait_recv()
    for i in range(2):
        for part in range(2):
            wo_load(i, part).wait()

    def out_conv_step(n, carry):
        cols = pl.ds(pl.multiple_of(n * 512, 512), 512)
        oacc[:, cols] = mm(cob[own_rows, :], wob[0, 0, :, cols]) + mm(
            cor[...], wob[0, 1, :, cols]
        )
        return carry

    lax.fori_loop(0, 4, out_conv_step, 0)

    for k in range(6):
        second[k].wait_recv()
    down = [
        jnp.where(i < z, jnp.exp(rows_between(i) + before_me), 0.0) for i in range(4)
    ]
    for h in range(HEADS):
        j = h % 2
        if h < 2:
            state = pre[j]
            for i in range(4):
                state = state + lane_row(down[i], h) * a2[i, j].astype(F32)
        else:
            state = b2[0, j].astype(F32)
            for i in range(1, 4):
                state = state + b2[i, j].astype(F32)
        for b in range(BLOCKS):
            starts[b, h] = state.astype(BF16)
            if b < BLOCKS - 1:
                state = jnp.exp(block_end(b, h)) * state + states[b, h]

    def across(first):
        def step(i, carry):
            b = first + i
            rows = pl.ds(pl.multiple_of(b * 128, 128), 128)
            for h in range(HEADS):
                at = slice(h * 128, h * 128 + 128)
                value = inside[rows, at] + jnp.exp(colrep[b, h]) * mm(
                    qb[rows, at], starts[b, h]
                )
                level = jnp.mean(value * value, axis=1, keepdims=True)
                retb[rows, at] = (value * lax.rsqrt(level + EPS)).astype(BF16)
            return carry

        lax.fori_loop(0, 3, step, 0)

    across(other * 3)
    ret_send = remote(retb.at[far_rows, :], retr, rs, rr, {"tp": other})
    ret_send.start()
    across(tp * 3)

    def out_near_step(n, carry):
        cols = pl.ds(pl.multiple_of(n * 512, 512), 512)
        oacc[:, cols] += mm(retb[own_rows, :], wob[1, 0, :, cols])
        return carry

    lax.fori_loop(0, 4, out_near_step, 0)
    ret_send.wait_recv()

    def out_far_step(n, carry):
        cols = pl.ds(pl.multiple_of(n * 512, 512), 512)
        out[:, cols] = (oacc[:, cols] + mm(retr[...], wob[1, 1, :, cols])).astype(BF16)
        return carry

    lax.fori_loop(0, 4, out_far_step, 0)

    for copy in [pack_send] + tok_send + l1_send + l2_send + exchange + second + [halo, conv_send, ret_send]:
        copy.wait_send()


def body(
    tokens, norm_gain, w_query, w_key, w_value, log_decay, w_conv_in, w_conv_pre,
    w_conv_post, conv_taps, w_out_ret, w_out_conv,
):
    within, bases = rotation_tables(16)
    dma = pltpu.SemaphoreType.DMA
    v = pltpu.VMEM
    scratch = [
        v((ROWS, KW), BF16), v((ROWS, KW), BF16), v((ROWS, KW), BF16),
        v((6, 2, KW, NW), BF16), v((2, 2, NW, D), BF16), v((4, ROWS, NW), F32),
        v((ROWS, NW), BF16), v((ROWS, NW), BF16), v((ROWS, NW), BF16),
        v((ROWS, NW), BF16), v((ROWS, NW), BF16), v((4, ROWS + 8, 128), F32),
        v((ROWS, NW), BF16), v((HALF, NW), BF16), v((ROWS, NW), BF16), v((HALF, NW), BF16),
        v((ROWS, NW), F32), v((BLOCKS, HEADS, 128, 128), F32),
        v((BLOCKS, HEADS, 128, 128), BF16), v((HALF, D), F32),
        v((ROWS, 128), F32), v((128, 128), F32), v((128, 128), F32),
        v((ROWS, 128), F32), v((ROWS, 128), F32),
        v((4, 128, 128), F32), v((16, 128), F32), v((1, D), BF16), v((HEADS, ROWS), F32),
        v((3, NW), BF16), v((128, 128), F32), v((128, 128), F32),
        v((BLOCKS, HEADS, 128, 128), F32), v((4, 8, 128), F32), v((4, 2, 8, 128), F32),
        v((4, 2, 128, 128), BF16), v((4, 2, 128, 128), BF16),
        v((4, 2, 128, 128), BF16), v((4, 2, 128, 128), BF16),
        v((3, 2, 128, 128), BF16), v((2, 128, 128), F32),
        dma((3,)), dma((5,)), dma((12,)), dma((4,)),
    ] + [dma((3,))] * 14 + [dma] * 8
    anywhere = pl.BlockSpec(memory_space=pl.ANY)
    return pl.pallas_call(
        kernel,
        out_shape=jax.ShapeDtypeStruct((HALF, D), BF16),
        in_specs=[anywhere] * 14,
        out_specs=pl.BlockSpec(memory_space=pltpu.VMEM),
        scratch_shapes=scratch,
        compiler_params=pltpu.CompilerParams(
            collective_id=0, has_side_effects=True, vmem_limit_bytes=62 * 1024 * 1024
        ),
    )(
        tokens, norm_gain.reshape(1, D), log_decay, conv_taps, w_key, w_value, w_query,
        w_conv_in, w_conv_pre, w_conv_post, w_out_conv, w_out_ret,
        jnp.asarray(within), jnp.asarray(bases),
    )


def solution(mesh):
    in_specs = (
        P(("fs", "sp"), "tp"),
        P(),
        P(None, "tp"),
        P(None, "tp"),
        P(None, "tp"),
        P("tp", "sp"),
        P(None, "tp"),
        P(None, "tp"),
        P(None, "tp"),
        P(None, "tp"),
        P(),
        P(),
    )
    out_specs = P(("fs", "sp", "tp"), None)
    return jax.shard_map(body, mesh=mesh, in_specs=in_specs, out_specs=out_specs, check_vma=False)
```

```python
import functools

import jax
import jax.numpy as jnp
import numpy as np
from jax import lax
from jax.experimental import pallas as pl
from jax.experimental.pallas import tpu as pltpu
from jax.sharding import PartitionSpec as P

DH = 128
SPAN = 128
ROWS = 768
HALF = 384
BLOCKS = 6
HEADS = 4
KW = 1024
NW = 512
D = 2048
EPS = 1e-06
KEY_SCALE = 128.0 ** -0.5
F32 = jnp.float32
BF16 = jnp.bfloat16
MESH = pl.DeviceIdType.MESH
WEIGHTS = ("wk", "wv", "wq", "wci", "wcp", "wcq")


def rotation_tables(places):
    half = DH // 2
    rate = 10000.0 ** (-np.arange(half, dtype=np.float64) / half)
    inner = np.arange(SPAN, dtype=np.float64)[:, None] * rate[None, :]
    inner = np.concatenate([inner, inner], axis=1)
    sign = np.concatenate([-np.ones(half), np.ones(half)])[None, :]
    within = np.stack(
        [np.cos(inner), np.sin(inner), sign * np.cos(inner), sign * np.sin(inner)]
    ).astype(np.float32)
    start = np.arange(places * BLOCKS, dtype=np.float64) * SPAN
    outer = start[:, None] * rate[None, :]
    outer = np.concatenate([outer, outer], axis=1).reshape(places, BLOCKS, DH)
    bases = np.zeros((places, 16, DH), np.float32)
    bases[:, :BLOCKS] = np.cos(outer)
    bases[:, 8 : 8 + BLOCKS] = np.sin(outer)
    return within, bases


def mm(a, b):
    return jnp.dot(a, b, preferred_element_type=F32)


def kernel(
    tok, gain, ld, taps, wk, wv, wq, wci, wcp, wcq, woc, wor, tabs, bases,
    out,
    xo, go, gp, wbuf, wob, acc, kb, vb, qb, cib, postb, gbuf, cob, cor,
    retb, retr, inside, starts, oacc, ssb, pack, pack_far, rot_c, rot_s,
    tabv, basev, gainv, ldv, tapv, ldp, cumr, colrep, lrow, lcol,
    a1, a2, b1, b2, bm, pre, fade, tails, cumc, endr, qs, entry, both,
    sem_tok, sem_small, sem_w, sem_wo,
    ts, tr, l1s, l1r, l2s, l2r, a1s, a1r, a2s, a2r, b1s, b1r, b2s, b2r,
    hs, hr, cs, cr, rs, rr, ps, pr,
):
    sp = lax.axis_index("sp")
    tp = lax.axis_index("tp")
    x = lax.rem(sp, 4)
    z = lax.div(sp, 4)
    other = 1 - tp
    row_peer = [z * 4 + lax.rem(x + k, 4) for k in (1, 2, 3)]
    col_peer = [lax.rem(z + k, 4) * 4 + x for k in (1, 2, 3)]
    after = lax.rem(sp + 1, 16)
    before = lax.rem(sp + 15, 16)

    barrier = pltpu.get_barrier_semaphore()
    pl.semaphore_signal(barrier, inc=1, device_id={"tp": other}, device_id_type=MESH)
    for peer in row_peer + col_peer + [after, before]:
        pl.semaphore_signal(barrier, inc=1, device_id={"sp": peer}, device_id_type=MESH)

    def remote(src, dst, send, recv, where):
        return pltpu.make_async_remote_copy(
            src_ref=src, dst_ref=dst, send_sem=send, recv_sem=recv,
            device_id=where, device_id_type=MESH,
        )

    own_k = pl.multiple_of(tp * KW, KW)
    far_k = pl.multiple_of(other * KW, KW)
    own_n = pl.multiple_of(tp * NW, NW)
    far_n = pl.multiple_of(other * NW, NW)
    own_rows = pl.ds(pl.multiple_of(tp * HALF, HALF), HALF)
    far_rows = pl.ds(pl.multiple_of(other * HALF, HALF), HALF)

    tok_load = [
        pltpu.make_async_copy(
            tok.at[pl.ds(c * 256, 256), :], xo.at[pl.ds(c * 256, 256), :], sem_tok.at[c]
        )
        for c in range(3)
    ]
    small = [
        pltpu.make_async_copy(ld, ldv, sem_small.at[0]),
        pltpu.make_async_copy(gain, gainv, sem_small.at[1]),
        pltpu.make_async_copy(taps, tapv, sem_small.at[2]),
        pltpu.make_async_copy(tabs, tabv, sem_small.at[3]),
        pltpu.make_async_copy(bases.at[sp], basev, sem_small.at[4]),
    ]
    hbm = dict(zip(WEIGHTS, (wk, wv, wq, wci, wcp, wcq)))
    index = {name: i for i, name in enumerate(WEIGHTS)}

    def w_load(name, part):
        i = index[name]
        rows = pl.ds(own_k if part == 0 else far_k, KW)
        return pltpu.make_async_copy(
            hbm[name].at[rows, :], wbuf.at[i, part], sem_w.at[i * 2 + part]
        )

    def wo_load(i, part):
        rows = pl.ds(own_n if part == 0 else far_n, NW)
        return pltpu.make_async_copy(
            (woc, wor)[i].at[rows, :], wob.at[i, part], sem_wo.at[i * 2 + part]
        )

    small[0].start()
    small[1].start()
    for copy in tok_load:
        copy.start()
    w_load("wk", 0).start()
    w_load("wv", 0).start()
    small[4].start()
    small[3].start()
    small[2].start()

    lane = lax.broadcasted_iota(jnp.int32, (SPAN, SPAN), 1)
    packed = jnp.zeros((SPAN, SPAN), F32)
    for i in range(BLOCKS):
        if i % 2 == 0:
            tok_load[i // 2].wait()
        rows = slice(i * 128, i * 128 + 128)
        value = xo[rows, :].astype(F32)
        squares = jnp.sum(value * value, axis=1, keepdims=True)
        spread = jnp.broadcast_to(squares, (SPAN, SPAN))
        ssb[rows, :] = spread
        packed = jnp.where(lane == i, spread, packed)
    pack[...] = packed

    pl.semaphore_wait(barrier, 9)
    pack_send = remote(pack, pack_far, ps, pr, {"tp": other})
    pack_send.start()
    ldp[...] = jnp.zeros_like(ldp)
    small[0].wait()
    for b in range(BLOCKS):
        ldp[b * 8 : b * 8 + HEADS, :] = ldv[:, b * SPAN : (b + 1) * SPAN]
    upper = (
        lax.broadcasted_iota(jnp.int32, (SPAN, SPAN), 0)
        <= lax.broadcasted_iota(jnp.int32, (SPAN, SPAN), 1)
    )
    ones = jnp.where(upper, 1.0, 0.0).astype(BF16)
    rest = ldp[...]
    total = jnp.zeros((SPAN, SPAN), F32)
    for _ in range(3):
        piece = rest.astype(BF16)
        total = total + mm(piece, ones)
        rest = rest - piece.astype(F32)
    cumr[...] = total
    cumc[...] = total.T
    ends = jnp.broadcast_to(total[:, SPAN - 1 : SPAN], (SPAN, SPAN))
    endr[...] = ends
    whole = ends[0:8]
    for b in range(1, BLOCKS):
        whole = whole + ends[b * 8 : b * 8 + 8]
    lrow[x] = whole

    def block_end(b, h):
        return endr[b * 8 + h : b * 8 + h + 1, :]

    def section(body):
        pl.when(sp < 16)(body)

    l1_send = [
        remote(lrow.at[x], lrow.at[x], l1s.at[k], l1r.at[k], {"sp": row_peer[k]})
        for k in range(3)
    ]
    for copy in l1_send:
        copy.start()
    w_load("wq", 0).start()

    small[1].wait()
    weight = gainv[pl.ds(own_k, KW)].astype(F32).reshape(1, KW)
    pack_send.wait_recv()
    tok_send = [
        remote(
            go.at[pl.ds(c * 256, 256), :], gp.at[pl.ds(c * 256, 256), :],
            ts.at[c], tr.at[c], {"tp": other},
        )
        for c in range(3)
    ]
    for i in range(BLOCKS):
        rows = slice(i * 128, i * 128 + 128)
        level = ssb[rows, :] + jnp.broadcast_to(pack_far[:, i : i + 1], (SPAN, SPAN))
        scale = lax.rsqrt(level * (1.0 / D) + EPS)
        for c in range(KW // 128):
            at = slice(c * 128, c * 128 + 128)
            go[rows, at] = (xo[rows, at].astype(F32) * scale * weight[:, at]).astype(BF16)
        if i in (2, 4):
            tok_send[i // 2 - 1].start()
    tok_send[2].start()

    lower = (
        lax.broadcasted_iota(jnp.int32, (SPAN, SPAN), 0)
        >= lax.broadcasted_iota(jnp.int32, (SPAN, SPAN), 1)
    )

    def near_product(i):
        for n in range(2):
            cols = slice(n * 256, n * 256 + 256)
            acc[i, :, cols] = mm(go[...], wbuf[i, 0, :, cols])

    for name in ("wk", "wv", "wq"):
        w_load(name, 0).wait()
    for name in ("wk", "wv", "wq"):
        w_load(name, 1).start()
    for name in ("wci", "wcp"):
        for part in range(2):
            w_load(name, part).start()
    small[3].wait()
    small[4].wait()

    @section
    def _():
        near_product(0)
        for b in range(BLOCKS):
            rows = slice(b * 128, b * 128 + 128)
            base_c = basev[b : b + 1, :]
            base_s = basev[b + 8 : b + 9, :]
            rot_c[rows, :] = base_c * tabv[0] - base_s * tabv[1]
            rot_s[rows, :] = base_s * tabv[2] + base_c * tabv[3]
        near_product(1)
        for b in range(BLOCKS):
            for h in range(HEADS):
                i = b * 8 + h
                column = jnp.broadcast_to(cumc[:, i : i + 1], (SPAN, SPAN))
                colrep[b, h] = column
                gap = column - cumr[i : i + 1, :]
                fade[b, h] = jnp.where(lower, jnp.exp(jnp.minimum(gap, 0.0)), 0.0)
                tails[b, h] = jnp.exp(block_end(b, h) - column)
        near_product(2)

    for copy in l1_send:
        copy.wait_recv()
    line = [lrow[i] for i in range(4)]

    def between(low, high):
        parts = [
            jnp.where(jnp.logical_and(i > low, i < high), line[i], 0.0) for i in range(4)
        ]
        return (parts[0] + parts[1]) + (parts[2] + parts[3])

    row_total = (line[0] + line[1]) + (line[2] + line[3])
    lcol[z, 0] = row_total
    lcol[z, 1] = between(x, 4)
    l2_send = [
        remote(lcol.at[z], lcol.at[z], l2s.at[k], l2r.at[k], {"sp": col_peer[k]})
        for k in range(3)
    ]
    for copy in l2_send:
        copy.start()

    for copy in tok_send:
        copy.wait_recv()

    def rotated(value):
        return value * rot_c[...] + pltpu.roll(value, 64, axis=1) * rot_s[...]

    exchange = []

    def key_value(n):
        cols = slice(n * 256, n * 256 + 256)
        kk = acc[0, :, cols] + mm(gp[...], wbuf[0, 1, :, cols])
        for j in range(2):
            at = slice(n * 256 + j * 128, n * 256 + j * 128 + 128)
            kb[:, at] = (rotated(kk[:, j * 128 : j * 128 + 128]) * KEY_SCALE).astype(BF16)
        vv = acc[1, :, cols] + mm(gp[...], wbuf[1, 1, :, cols])
        vb[:, cols] = vv.astype(BF16)

    def fresh_states(n):
        slot = a1.at[x] if n == 0 else b1.at[z]
        for j in range(2):
            h = n * 2 + j
            at = slice(h * 128, h * 128 + 128)
            whole = None
            for b in range(BLOCKS):
                rows = slice(b * 128, b * 128 + 128)
                weighted = (vb[rows, at].astype(F32) * tails[b, h]).astype(BF16)
                fresh = lax.dot_general(
                    kb[rows, at], weighted, (((0,), (0,)), ((), ())),
                    preferred_element_type=F32,
                )
                if b == 0:
                    whole = fresh
                else:
                    starts[b, h] = whole.astype(BF16)
                    whole = jnp.exp(block_end(b, h)) * whole + fresh
            slot[j] = whole.astype(BF16)

    def send_states(n):
        for k in range(3):
            if n == 0:
                copy = remote(a1.at[x], a1.at[x], a1s.at[k], a1r.at[k], {"sp": row_peer[k]})
            else:
                copy = remote(b1.at[z], b1.at[z], b1s.at[k], b1r.at[k], {"sp": col_peer[k]})
            copy.start()
            exchange.append(copy)

    for name in ("wk", "wv", "wq"):
        w_load(name, 1).wait()
    @section
    def _():
        key_value(0)
        key_value(1)

    @section
    def _():
        fresh_states(0)
        fresh_states(1)

    send_states(0)
    send_states(1)

    for name in ("wci", "wcp"):
        for part in range(2):
            w_load(name, part).wait()
    for part in range(2):
        w_load("wcq", part).start()
    for i in range(2):
        for part in range(2):
            wo_load(i, part).start()

    def full_product(i, cols):
        return (
            mm(go[...], wbuf[i, 0, :, cols]) + mm(gp[...], wbuf[i, 1, :, cols])
        ).astype(BF16)

    @section
    def _():
        for n in range(2):
            cols = slice(n * 256, n * 256 + 256)
            cib[:, cols] = full_product(3, cols)
            gated = full_product(4, cols).astype(F32) * cib[:, cols].astype(F32)
            gated = gated.astype(BF16).astype(F32)
            for j in range(2):
                gbuf[n * 2 + j, 8 : 8 + ROWS, :] = gated[:, j * 128 : j * 128 + 128]

    halo = remote(
        gbuf.at[:, pl.ds(ROWS, 8), :], gbuf.at[:, pl.ds(0, 8), :], hs, hr, {"sp": after}
    )
    halo.start()

    @section
    def _():
        for n in range(2):
            cols = slice(n * 256, n * 256 + 256)
            qq = acc[2, :, cols] + mm(gp[...], wbuf[2, 1, :, cols])
            for j in range(2):
                at = slice(n * 256 + j * 128, n * 256 + j * 128 + 128)
                qb[:, at] = rotated(qq[:, j * 128 : j * 128 + 128]).astype(BF16)


    for copy in l2_send:
        copy.wait_recv()
    row_sums = [lcol[i, 0] for i in range(4)]
    suffix = [lcol[i, 1] for i in range(4)]
    before_me = between(-1, x)

    def rows_between(low):
        parts = [
            jnp.where(jnp.logical_and(i > low, i < z), row_sums[i], 0.0) for i in range(4)
        ]
        return (parts[0] + parts[1]) + (parts[2] + parts[3])

    def lane_row(weight, h):
        return weight[h : h + 1, :]

    to_end = [jnp.exp(between(i, 4)) for i in range(4)]
    to_me = [jnp.where(i < x, jnp.exp(between(i, x)), 0.0) for i in range(4)]
    for k in range(3):
        exchange[k].wait_recv()
    for j in range(2):
        parts = [a1[i, j].astype(F32) for i in range(4)]
        row_state = lane_row(to_end[0], j) * parts[0]
        prefix = lane_row(to_me[0], j) * parts[0]
        for i in range(1, 4):
            row_state = row_state + lane_row(to_end[i], j) * parts[i]
            prefix = prefix + lane_row(to_me[i], j) * parts[i]
        pre[j] = prefix
        a2[z, j] = row_state.astype(BF16)
    second = []
    for k in range(3):
        copy = remote(a2.at[z], a2.at[z], a2s.at[k], a2r.at[k], {"sp": col_peer[k]})
        copy.start()
        second.append(copy)
    above = [
        jnp.where(i < z, jnp.exp(suffix[i] + rows_between(i)), 0.0) for i in range(4)
    ]
    for k in range(3):
        exchange[3 + k].wait_recv()
    e_own = jnp.exp(before_me)
    for j in range(2):
        h = 2 + j
        column = lane_row(above[0], h) * b1[0, j].astype(F32)
        for i in range(1, 4):
            column = column + lane_row(above[i], h) * b1[i, j].astype(F32)
        mine = b1[z, j].astype(F32)
        b2[x, j] = (lane_row(e_own, h) * column).astype(BF16)
        for k in range(3):
            target = lax.rem(x + k + 1, 4)
            e_col = jnp.exp(between(-1, target))
            e_mine = jnp.where(x < target, jnp.exp(between(x, target)), 0.0)
            bm[k, j] = (lane_row(e_col, h) * column + lane_row(e_mine, h) * mine).astype(BF16)
    for k in range(3):
        copy = remote(bm.at[k], b2.at[x], b2s.at[k], b2r.at[k], {"sp": row_peer[k]})
        copy.start()
        second.append(copy)

    for part in range(2):
        w_load("wcq", part).wait()
    @section
    def _():
        for n in range(2):
            cols = slice(n * 256, n * 256 + 256)
            postb[:, cols] = full_product(5, cols)

    small[2].wait()
    halo.wait_recv()

    @pl.when(sp == 0)
    def _():
        gbuf[:, 0:8, :] = jnp.zeros((4, 8, 128), F32)

    @section
    def _():
        for c in range(4):
            at = slice(c * 128, c * 128 + 128)
            summed = jnp.zeros((ROWS, 128), F32)
            for i in range(3):
                summed = summed + tapv[i : i + 1, at].astype(F32) * gbuf[c, 6 + i : 6 + i + ROWS, :]
            cob[:, at] = (postb[:, at].astype(F32) * summed).astype(BF16)

    conv_send = remote(cob.at[far_rows, :], cor, cs, cr, {"tp": other})
    conv_send.start()

    @section
    def _():
        for b in range(BLOCKS):
            rows = slice(b * 128, b * 128 + 128)
            for h in range(HEADS):
                at = slice(h * 128, h * 128 + 128)
                scores = lax.dot_general(
                    qb[rows, at], kb[rows, at], (((1,), (1,)), ((), ())),
                    preferred_element_type=F32,
                )
                both[b, h, :, :128] = (scores * fade[b, h]).astype(BF16)
                query = qb[rows, at].astype(F32)
                if b == 0:
                    qs[rows, at] = (query * jnp.exp(colrep[b, h])).astype(BF16)
                else:
                    both[b, h, :, 128:] = (query * jnp.exp(colrep[b, h])).astype(BF16)
                    offset = endr[h : h + 1, :]
                    for e in range(1, b):
                        offset = offset + block_end(e, h)
                    qs[rows, at] = (query * jnp.exp(colrep[b, h] + offset)).astype(BF16)
        for b in range(BLOCKS):
            rows = slice(b * 128, b * 128 + 128)
            for h in range(HEADS):
                at = slice(h * 128, h * 128 + 128)
                if b == 0:
                    inside[rows, at] = mm(both[b, h, :, :128], vb[rows, at])
                else:
                    inside[rows, at] = mm(
                        both[b, h],
                        jnp.concatenate([vb[rows, at], starts[b, h]], axis=0),
                    )

    for i in range(2):
        for part in range(2):
            wo_load(i, part).wait()
    conv_send.wait_recv()

    @section
    def _():
        for n in range(8):
            cols = slice(n * 256, n * 256 + 256)
            oacc[:, cols] = mm(cob[own_rows, :], wob[0, 0, :, cols]) + mm(
                cor[...], wob[0, 1, :, cols]
            )

    for k in range(6):
        second[k].wait_recv()
    down = [
        jnp.where(i < z, jnp.exp(rows_between(i) + before_me), 0.0) for i in range(4)
    ]
    for h in range(HEADS):
        j = h % 2
        if h < 2:
            state = pre[j]
            for i in range(4):
                state = state + lane_row(down[i], h) * a2[i, j].astype(F32)
        else:
            state = b2[0, j].astype(F32)
            for i in range(1, 4):
                state = state + b2[i, j].astype(F32)
        entry[h] = state.astype(BF16)

    def across(first):
        for i in range(3):
            rows = pl.ds(pl.multiple_of(first + i * 128, 128), 128)
            for h in range(HEADS):
                at = slice(h * 128, h * 128 + 128)
                value = inside[rows, at] + mm(qs[rows, at], entry[h])
                level = jnp.mean(value * value, axis=1, keepdims=True)
                retb[rows, at] = (value * lax.rsqrt(level + EPS)).astype(BF16)

    section(lambda: across(other * HALF))
    ret_send = remote(retb.at[far_rows, :], retr, rs, rr, {"tp": other})
    ret_send.start()
    section(lambda: across(tp * HALF))

    @section
    def _():
        for n in range(8):
            cols = slice(n * 256, n * 256 + 256)
            oacc[:, cols] += mm(retb[own_rows, :], wob[1, 0, :, cols])

    ret_send.wait_recv()

    @section
    def _():
        for n in range(8):
            cols = slice(n * 256, n * 256 + 256)
            out[:, cols] = (oacc[:, cols] + mm(retr[...], wob[1, 1, :, cols])).astype(BF16)

    for copy in [pack_send] + tok_send + l1_send + l2_send + exchange + second + [halo, conv_send, ret_send]:
        copy.wait_send()


def body(
    tokens, norm_gain, w_query, w_key, w_value, log_decay, w_conv_in, w_conv_pre,
    w_conv_post, conv_taps, w_out_ret, w_out_conv,
):
    within, bases = rotation_tables(16)
    dma = pltpu.SemaphoreType.DMA
    v = pltpu.VMEM
    scratch = [
        v((ROWS, KW), BF16), v((ROWS, KW), BF16), v((ROWS, KW), BF16),
        v((6, 2, KW, NW), BF16), v((2, 2, NW, D), BF16), v((3, ROWS, NW), F32),
        v((ROWS, NW), BF16), v((ROWS, NW), BF16), v((ROWS, NW), BF16),
        v((ROWS, NW), BF16), v((ROWS, NW), BF16), v((4, ROWS + 8, 128), F32),
        v((ROWS, NW), BF16), v((HALF, NW), BF16), v((ROWS, NW), BF16), v((HALF, NW), BF16),
        v((ROWS, NW), F32),
        v((BLOCKS, HEADS, 128, 128), BF16), v((HALF, D), F32),
        v((ROWS, 128), F32), v((128, 128), F32), v((128, 128), F32),
        v((ROWS, 128), F32), v((ROWS, 128), F32),
        v((4, 128, 128), F32), v((16, 128), F32), v((D,), BF16), v((HEADS, ROWS), F32),
        v((3, NW), BF16), v((128, 128), F32), v((128, 128), F32),
        v((BLOCKS, HEADS, 128, 128), F32), v((4, 8, 128), F32), v((4, 2, 8, 128), F32),
        v((4, 2, 128, 128), BF16), v((4, 2, 128, 128), BF16),
        v((4, 2, 128, 128), BF16), v((4, 2, 128, 128), BF16),
        v((3, 2, 128, 128), BF16), v((2, 128, 128), F32),
        v((BLOCKS, HEADS, 128, 128), F32), v((BLOCKS, HEADS, 128, 128), F32),
        v((128, 128), F32), v((128, 128), F32), v((ROWS, NW), BF16), v((HEADS, 128, 128), BF16),
        v((BLOCKS, HEADS, 128, 256), BF16),
        dma((3,)), dma((5,)), dma((12,)), dma((4,)),
    ] + [dma((3,))] * 14 + [dma] * 8
    anywhere = pl.BlockSpec(memory_space=pltpu.HBM)
    return pl.pallas_call(
        kernel,
        out_shape=pltpu.VMEM((HALF, D), BF16),
        in_specs=[anywhere] * 14,
        out_specs=pl.BlockSpec(memory_space=pltpu.VMEM),
        scratch_shapes=scratch,
        compiler_params=pltpu.CompilerParams(
            collective_id=0, has_side_effects=True, vmem_limit_bytes=56 * 1024 * 1024
        ),
    )(
        tokens, norm_gain, log_decay, conv_taps, w_key, w_value, w_query,
        w_conv_in, w_conv_pre, w_conv_post, w_out_conv, w_out_ret,
        jnp.asarray(within), jnp.asarray(bases),
    )


def solution(mesh):
    in_specs = (
        P(("fs", "sp"), "tp"),
        P(),
        P(None, "tp"),
        P(None, "tp"),
        P(None, "tp"),
        P("tp", "sp"),
        P(None, "tp"),
        P(None, "tp"),
        P(None, "tp"),
        P(None, "tp"),
        P(),
        P(),
    )
    out_specs = P(("fs", "sp", "tp"), None)
    return jax.shard_map(body, mesh=mesh, in_specs=in_specs, out_specs=out_specs, check_vma=False)
```

```python
import functools

import jax
import jax.numpy as jnp
import numpy as np
from jax import lax
from jax.experimental import pallas as pl
from jax.experimental.pallas import tpu as pltpu
from jax.sharding import PartitionSpec as P

DH = 128
SPAN = 128
ROWS = 768
HALF = 384
BLOCKS = 6
HEADS = 4
KW = 1024
NW = 512
D = 2048
EPS = 1e-06
KEY_SCALE = 128.0 ** -0.5
F32 = jnp.float32
BF16 = jnp.bfloat16
MESH = pl.DeviceIdType.MESH
WEIGHTS = ("wk", "wv", "wq", "wci", "wcp", "wcq")


def rotation_tables(places):
    half = DH // 2
    rate = 10000.0 ** (-np.arange(half, dtype=np.float64) / half)
    inner = np.arange(SPAN, dtype=np.float64)[:, None] * rate[None, :]
    inner = np.concatenate([inner, inner], axis=1)
    sign = np.concatenate([-np.ones(half), np.ones(half)])[None, :]
    within = np.stack(
        [np.cos(inner), np.sin(inner), sign * np.cos(inner), sign * np.sin(inner)]
    ).astype(np.float32)
    start = np.arange(places * BLOCKS, dtype=np.float64) * SPAN
    outer = start[:, None] * rate[None, :]
    outer = np.concatenate([outer, outer], axis=1).reshape(places, BLOCKS, DH)
    bases = np.zeros((places, 16, DH), np.float32)
    bases[:, :BLOCKS] = np.cos(outer)
    bases[:, 8 : 8 + BLOCKS] = np.sin(outer)
    return within, bases


def mm(a, b):
    return jnp.dot(a, b, preferred_element_type=F32)


def kernel(
    tok, gain, ld, taps, wk, wv, wq, wci, wcp, wcq, woc, wor, tabs, bases,
    out,
    xo, go, gp, wbuf, wob, acc, kb, vb, qb, cib, postb, gbuf, cob, cor,
    retb, retr, inside, starts, oacc, ssb, pack, pack_far, rot_c, rot_s,
    tabv, basev, gainv, ldv, tapv, ldp, cumr, colrep, lall,
    a1, a2, b1, b2, bm, pre, fade, tails, cumc, endr, qs, entry, both,
    sem_tok, sem_small, sem_w, sem_wo,
    ts, tr, ls, lr, a1s, a1r, a2s, a2r, b1s, b1r, b2s, b2r,
    hs, hr, cs, cr, rs, rr, ps, pr, met,
):
    sp = lax.axis_index("sp")
    tp = lax.axis_index("tp")
    x = lax.rem(sp, 4)
    z = lax.div(sp, 4)
    other = 1 - tp
    row_peer = [z * 4 + lax.rem(x + k, 4) for k in (1, 2, 3)]
    col_peer = [lax.rem(z + k, 4) * 4 + x for k in (1, 2, 3)]
    after = lax.rem(sp + 1, 16)
    ahead = [lax.rem(sp + k, 16) for k in range(1, 16)]
    behind = [lax.rem(sp + 16 - k, 16) for k in range(1, 16)]

    barrier = pltpu.get_barrier_semaphore()
    lall[...] = jnp.zeros_like(lall)
    a2[...] = jnp.zeros_like(a2)
    b1[...] = jnp.zeros_like(b1)

    @pl.when(tp == 0)
    def _():
        pl.semaphore_signal(barrier, inc=1, device_id={"tp": 1}, device_id_type=MESH)

    def remote(src, dst, send, recv, where):
        return pltpu.make_async_remote_copy(
            src_ref=src, dst_ref=dst, send_sem=send, recv_sem=recv,
            device_id=where, device_id_type=MESH,
        )

    own_k = pl.multiple_of(tp * KW, KW)
    far_k = pl.multiple_of(other * KW, KW)
    own_n = pl.multiple_of(tp * NW, NW)
    far_n = pl.multiple_of(other * NW, NW)
    own_rows = pl.ds(pl.multiple_of(tp * HALF, HALF), HALF)
    far_rows = pl.ds(pl.multiple_of(other * HALF, HALF), HALF)

    tok_load = [
        pltpu.make_async_copy(
            tok.at[pl.ds(c * 256, 256), :], xo.at[pl.ds(c * 256, 256), :], sem_tok.at[c]
        )
        for c in range(3)
    ]
    small = [
        pltpu.make_async_copy(ld, ldv, sem_small.at[0]),
        pltpu.make_async_copy(gain, gainv, sem_small.at[1]),
        pltpu.make_async_copy(taps, tapv, sem_small.at[2]),
        pltpu.make_async_copy(tabs, tabv, sem_small.at[3]),
        pltpu.make_async_copy(bases.at[sp], basev, sem_small.at[4]),
    ]
    hbm = dict(zip(WEIGHTS, (wk, wv, wq, wci, wcp, wcq)))
    index = {name: i for i, name in enumerate(WEIGHTS)}

    def w_load(name, part):
        i = index[name]
        rows = pl.ds(own_k if part == 0 else far_k, KW)
        return pltpu.make_async_copy(
            hbm[name].at[rows, :], wbuf.at[i, part], sem_w.at[i * 2 + part]
        )

    def wo_load(i, part):
        rows = pl.ds(own_n if part == 0 else far_n, NW)
        return pltpu.make_async_copy(
            (woc, wor)[i].at[rows, :], wob.at[i, part], sem_wo.at[i * 2 + part]
        )

    small[0].start()
    small[1].start()
    for copy in tok_load:
        copy.start()
    w_load("wk", 0).start()
    w_load("wv", 0).start()
    small[4].start()
    small[3].start()
    small[2].start()

    lane = lax.broadcasted_iota(jnp.int32, (SPAN, SPAN), 1)
    packed = jnp.zeros((SPAN, SPAN), F32)
    for i in range(BLOCKS):
        if i % 2 == 0:
            tok_load[i // 2].wait()
        rows = slice(i * 128, i * 128 + 128)
        value = xo[rows, :].astype(F32)
        squares = jnp.sum(value * value, axis=1, keepdims=True)
        spread = jnp.broadcast_to(squares, (SPAN, SPAN))
        ssb[rows, :] = spread
        packed = jnp.where(lane == i, spread, packed)
    pack[...] = packed

    @pl.when(tp == 1)
    def _():
        pl.semaphore_wait(barrier, 1)
        pl.semaphore_signal(met, inc=1, device_id={"tp": 0}, device_id_type=MESH)

    @pl.when(tp == 0)
    def _():
        pl.semaphore_wait(met, 1)
        for peer in ahead:
            pl.semaphore_signal(barrier, inc=1, device_id={"sp": peer}, device_id_type=MESH)

    pack_send = remote(pack, pack_far, ps, pr, {"tp": other})
    pack_send.start()
    ldp[...] = jnp.zeros_like(ldp)
    small[0].wait()
    for b in range(BLOCKS):
        ldp[b * 8 : b * 8 + HEADS, :] = ldv[:, b * SPAN : (b + 1) * SPAN]
    upper = (
        lax.broadcasted_iota(jnp.int32, (SPAN, SPAN), 0)
        <= lax.broadcasted_iota(jnp.int32, (SPAN, SPAN), 1)
    )
    ones = jnp.where(upper, 1.0, 0.0).astype(BF16)
    rest = ldp[...]
    total = jnp.zeros((SPAN, SPAN), F32)
    for _ in range(3):
        piece = rest.astype(BF16)
        total = total + mm(piece, ones)
        rest = rest - piece.astype(F32)
    cumr[...] = total
    cumc[...] = total.T
    ends = jnp.broadcast_to(total[:, SPAN - 1 : SPAN], (SPAN, SPAN))
    endr[...] = ends
    whole = ends[0:8]
    for b in range(1, BLOCKS):
        whole = whole + ends[b * 8 : b * 8 + 8]
    lall[sp] = whole

    def block_end(b, h):
        return endr[b * 8 + h : b * 8 + h + 1, :]

    def section(body):
        pl.when(sp < 16)(body)

    w_load("wq", 0).start()

    small[1].wait()
    weight = gainv[pl.ds(own_k, KW)].astype(F32).reshape(1, KW)
    pack_send.wait_recv()
    tok_send = [
        remote(
            go.at[pl.ds(c * 256, 256), :], gp.at[pl.ds(c * 256, 256), :],
            ts.at[c], tr.at[c], {"tp": other},
        )
        for c in range(3)
    ]
    for i in range(BLOCKS):
        rows = slice(i * 128, i * 128 + 128)
        level = ssb[rows, :] + jnp.broadcast_to(pack_far[:, i : i + 1], (SPAN, SPAN))
        scale = lax.rsqrt(level * (1.0 / D) + EPS)
        for c in range(KW // 128):
            at = slice(c * 128, c * 128 + 128)
            go[rows, at] = (xo[rows, at].astype(F32) * scale * weight[:, at]).astype(BF16)
        if i in (2, 4):
            tok_send[i // 2 - 1].start()
    tok_send[2].start()

    lower = (
        lax.broadcasted_iota(jnp.int32, (SPAN, SPAN), 0)
        >= lax.broadcasted_iota(jnp.int32, (SPAN, SPAN), 1)
    )

    def near_product(i):
        for n in range(2):
            cols = slice(n * 256, n * 256 + 256)
            acc[i, :, cols] = mm(go[...], wbuf[i, 0, :, cols])

    for name in ("wk", "wv", "wq"):
        w_load(name, 0).wait()
    for name in ("wk", "wv", "wq"):
        w_load(name, 1).start()
    for name in ("wci", "wcp"):
        for part in range(2):
            w_load(name, part).start()
    small[3].wait()
    small[4].wait()

    @section
    def _():
        near_product(0)
        for b in range(BLOCKS):
            rows = slice(b * 128, b * 128 + 128)
            base_c = basev[b : b + 1, :]
            base_s = basev[b + 8 : b + 9, :]
            rot_c[rows, :] = base_c * tabv[0] - base_s * tabv[1]
            rot_s[rows, :] = base_s * tabv[2] + base_c * tabv[3]
        near_product(1)
        for b in range(BLOCKS):
            for h in range(HEADS):
                i = b * 8 + h
                column = jnp.broadcast_to(cumc[:, i : i + 1], (SPAN, SPAN))
                colrep[b, h] = column
                gap = column - cumr[i : i + 1, :]
                fade[b, h] = jnp.where(lower, jnp.exp(jnp.minimum(gap, 0.0)), 0.0)
                tails[b, h] = jnp.exp(block_end(b, h) - column)
        near_product(2)

    for copy in tok_send:
        copy.wait_recv()

    def rotated(value):
        return value * rot_c[...] + pltpu.roll(value, 64, axis=1) * rot_s[...]

    exchange = []

    def key_value(n):
        cols = slice(n * 256, n * 256 + 256)
        kk = acc[0, :, cols] + mm(gp[...], wbuf[0, 1, :, cols])
        for j in range(2):
            at = slice(n * 256 + j * 128, n * 256 + j * 128 + 128)
            kb[:, at] = (rotated(kk[:, j * 128 : j * 128 + 128]) * KEY_SCALE).astype(BF16)
        vv = acc[1, :, cols] + mm(gp[...], wbuf[1, 1, :, cols])
        vb[:, cols] = vv.astype(BF16)

    def fresh_states(n):
        slot = a1.at[x] if n == 0 else b1.at[z]
        for j in range(2):
            h = n * 2 + j
            at = slice(h * 128, h * 128 + 128)
            whole = None
            for b in range(BLOCKS):
                rows = slice(b * 128, b * 128 + 128)
                weighted = (vb[rows, at].astype(F32) * tails[b, h]).astype(BF16)
                fresh = lax.dot_general(
                    kb[rows, at], weighted, (((0,), (0,)), ((), ())),
                    preferred_element_type=F32,
                )
                if b == 0:
                    whole = fresh
                else:
                    starts[b, h] = whole.astype(BF16)
                    whole = jnp.exp(block_end(b, h)) * whole + fresh
            slot[j] = whole.astype(BF16)

    def send_states(n):
        for k in range(3):
            if n == 0:
                copy = remote(a1.at[x], a1.at[x], a1s.at[k], a1r.at[k], {"sp": row_peer[k]})
            else:
                copy = remote(b1.at[z], b1.at[z], b1s.at[k], b1r.at[k], {"sp": col_peer[k]})
            pl.when(True if n == 0 else z + k < 3)(copy.start)
            exchange.append(copy)

    for name in ("wk", "wv", "wq"):
        w_load(name, 1).wait()
    @section
    def _():
        key_value(0)
        key_value(1)

    @pl.when(tp == 0)
    def _():
        pl.semaphore_wait(barrier, 15)
        pl.semaphore_signal(met, inc=1, device_id={"tp": 1}, device_id_type=MESH)

    @pl.when(tp == 1)
    def _():
        pl.semaphore_wait(met, 1)

    def total_copy(k):
        return remote(lall.at[sp], lall.at[sp], ls.at[k], lr.at[k], {"sp": ahead[k]})

    for k in range(15):
        pl.when(lax.div(ahead[k], 4) >= z)(total_copy(k).start)

    @section
    def _():
        fresh_states(0)
        fresh_states(1)

    send_states(0)
    send_states(1)

    for name in ("wci", "wcp"):
        for part in range(2):
            w_load(name, part).wait()
    for part in range(2):
        w_load("wcq", part).start()
    for i in range(2):
        for part in range(2):
            wo_load(i, part).start()

    def full_product(i, cols):
        return (
            mm(go[...], wbuf[i, 0, :, cols]) + mm(gp[...], wbuf[i, 1, :, cols])
        ).astype(BF16)

    @section
    def _():
        for n in range(2):
            cols = slice(n * 256, n * 256 + 256)
            cib[:, cols] = full_product(3, cols)
            gated = full_product(4, cols).astype(F32) * cib[:, cols].astype(F32)
            gated = gated.astype(BF16).astype(F32)
            for j in range(2):
                gbuf[n * 2 + j, 8 : 8 + ROWS, :] = gated[:, j * 128 : j * 128 + 128]

    halo = remote(
        gbuf.at[:, pl.ds(ROWS, 8), :], gbuf.at[:, pl.ds(0, 8), :], hs, hr, {"sp": after}
    )
    pl.when(sp < 15)(halo.start)

    @section
    def _():
        for n in range(2):
            cols = slice(n * 256, n * 256 + 256)
            qq = acc[2, :, cols] + mm(gp[...], wbuf[2, 1, :, cols])
            for j in range(2):
                at = slice(n * 256 + j * 128, n * 256 + j * 128 + 128)
                qb[:, at] = rotated(qq[:, j * 128 : j * 128 + 128]).astype(BF16)


    for k in range(15):
        pl.when(lax.div(behind[k], 4) <= z)(total_copy(k).wait_recv)
    totals = [[lall[4 * i + j] for j in range(4)] for i in range(4)]
    line = [lall[4 * z + j] for j in range(4)]

    def between(low, high):
        parts = [
            jnp.where(jnp.logical_and(i > low, i < high), line[i], 0.0) for i in range(4)
        ]
        return (parts[0] + parts[1]) + (parts[2] + parts[3])

    row_sums = [(t[0] + t[1]) + (t[2] + t[3]) for t in totals]
    suffix = []
    for t in totals:
        parts = [jnp.where(j > x, t[j], 0.0) for j in range(4)]
        suffix.append((parts[0] + parts[1]) + (parts[2] + parts[3]))
    before_me = between(-1, x)

    def rows_between(low):
        parts = [
            jnp.where(jnp.logical_and(i > low, i < z), row_sums[i], 0.0) for i in range(4)
        ]
        return (parts[0] + parts[1]) + (parts[2] + parts[3])

    def lane_row(weight, h):
        return weight[h : h + 1, :]

    second = []
    above = [
        jnp.where(i < z, jnp.exp(suffix[i] + rows_between(i)), 0.0) for i in range(4)
    ]
    for k in range(3):
        pl.when(z > k)(exchange[3 + k].wait_recv)
    e_own = jnp.exp(before_me)
    for j in range(2):
        h = 2 + j
        column = lane_row(above[0], h) * b1[0, j].astype(F32)
        for i in range(1, 4):
            column = column + lane_row(above[i], h) * b1[i, j].astype(F32)
        mine = b1[z, j].astype(F32)
        b2[x, j] = (lane_row(e_own, h) * column).astype(BF16)
        for k in range(3):
            target = lax.rem(x + k + 1, 4)
            e_col = jnp.exp(between(-1, target))
            e_mine = jnp.where(x < target, jnp.exp(between(x, target)), 0.0)
            bm[k, j] = (lane_row(e_col, h) * column + lane_row(e_mine, h) * mine).astype(BF16)
    for k in range(3):
        copy = remote(bm.at[k], b2.at[x], b2s.at[k], b2r.at[k], {"sp": row_peer[k]})
        copy.start()
        second.append(copy)

    for part in range(2):
        w_load("wcq", part).wait()
    @section
    def _():
        for n in range(2):
            cols = slice(n * 256, n * 256 + 256)
            postb[:, cols] = full_product(5, cols)

    to_end = [jnp.exp(between(i, 4)) for i in range(4)]
    to_me = [jnp.where(i < x, jnp.exp(between(i, x)), 0.0) for i in range(4)]
    for k in range(3):
        exchange[k].wait_recv()
    for j in range(2):
        parts = [a1[i, j].astype(F32) for i in range(4)]
        row_state = lane_row(to_end[0], j) * parts[0]
        prefix = lane_row(to_me[0], j) * parts[0]
        for i in range(1, 4):
            row_state = row_state + lane_row(to_end[i], j) * parts[i]
            prefix = prefix + lane_row(to_me[i], j) * parts[i]
        pre[j] = prefix
        a2[z, j] = row_state.astype(BF16)
    for k in range(3):
        copy = remote(a2.at[z], a2.at[z], a2s.at[k], a2r.at[k], {"sp": col_peer[k]})
        pl.when(z + k < 3)(copy.start)
        second.append(copy)

    small[2].wait()
    pl.when(sp > 0)(halo.wait_recv)

    @pl.when(sp == 0)
    def _():
        gbuf[:, 0:8, :] = jnp.zeros((4, 8, 128), F32)

    @section
    def _():
        for c in range(4):
            at = slice(c * 128, c * 128 + 128)
            summed = jnp.zeros((ROWS, 128), F32)
            for i in range(3):
                summed = summed + tapv[i : i + 1, at].astype(F32) * gbuf[c, 6 + i : 6 + i + ROWS, :]
            cob[:, at] = (postb[:, at].astype(F32) * summed).astype(BF16)

    conv_send = remote(cob.at[far_rows, :], cor, cs, cr, {"tp": other})
    conv_send.start()

    @section
    def _():
        for b in range(BLOCKS):
            rows = slice(b * 128, b * 128 + 128)
            for h in range(HEADS):
                at = slice(h * 128, h * 128 + 128)
                scores = lax.dot_general(
                    qb[rows, at], kb[rows, at], (((1,), (1,)), ((), ())),
                    preferred_element_type=F32,
                )
                both[b, h, :, :128] = (scores * fade[b, h]).astype(BF16)
                query = qb[rows, at].astype(F32)
                if b == 0:
                    qs[rows, at] = (query * jnp.exp(colrep[b, h])).astype(BF16)
                else:
                    both[b, h, :, 128:] = (query * jnp.exp(colrep[b, h])).astype(BF16)
                    offset = endr[h : h + 1, :]
                    for e in range(1, b):
                        offset = offset + block_end(e, h)
                    qs[rows, at] = (query * jnp.exp(colrep[b, h] + offset)).astype(BF16)
        for b in range(BLOCKS):
            rows = slice(b * 128, b * 128 + 128)
            for h in range(HEADS):
                at = slice(h * 128, h * 128 + 128)
                if b == 0:
                    inside[rows, at] = mm(both[b, h, :, :128], vb[rows, at])
                else:
                    inside[rows, at] = mm(
                        both[b, h],
                        jnp.concatenate([vb[rows, at], starts[b, h]], axis=0),
                    )

    for i in range(2):
        for part in range(2):
            wo_load(i, part).wait()
    conv_send.wait_recv()

    @section
    def _():
        for n in range(8):
            cols = slice(n * 256, n * 256 + 256)
            oacc[:, cols] = mm(cob[own_rows, :], wob[0, 0, :, cols]) + mm(
                cor[...], wob[0, 1, :, cols]
            )

    for k in range(3):
        second[k].wait_recv()
        pl.when(z > k)(second[3 + k].wait_recv)
    down = [
        jnp.where(i < z, jnp.exp(rows_between(i) + before_me), 0.0) for i in range(4)
    ]
    for h in range(HEADS):
        j = h % 2
        if h < 2:
            state = pre[j]
            for i in range(4):
                state = state + lane_row(down[i], h) * a2[i, j].astype(F32)
        else:
            state = b2[0, j].astype(F32)
            for i in range(1, 4):
                state = state + b2[i, j].astype(F32)
        entry[h] = state.astype(BF16)

    def across(first):
        for i in range(3):
            rows = pl.ds(pl.multiple_of(first + i * 128, 128), 128)
            for h in range(HEADS):
                at = slice(h * 128, h * 128 + 128)
                value = inside[rows, at] + mm(qs[rows, at], entry[h])
                level = jnp.mean(value * value, axis=1, keepdims=True)
                retb[rows, at] = (value * lax.rsqrt(level + EPS)).astype(BF16)

    section(lambda: across(other * HALF))
    ret_send = remote(retb.at[far_rows, :], retr, rs, rr, {"tp": other})
    ret_send.start()
    section(lambda: across(tp * HALF))

    @section
    def _():
        for n in range(8):
            cols = slice(n * 256, n * 256 + 256)
            oacc[:, cols] += mm(retb[own_rows, :], wob[1, 0, :, cols])

    ret_send.wait_recv()

    @section
    def _():
        for n in range(8):
            cols = slice(n * 256, n * 256 + 256)
            out[:, cols] = (oacc[:, cols] + mm(retr[...], wob[1, 1, :, cols])).astype(BF16)

    for copy in [pack_send, conv_send, ret_send] + tok_send + exchange[:3] + second[:3]:
        copy.wait_send()
    pl.when(sp < 15)(halo.wait_send)
    for k in range(3):
        pl.when(z + k < 3)(exchange[3 + k].wait_send)
        pl.when(z + k < 3)(second[3 + k].wait_send)
    for k in range(15):
        pl.when(lax.div(ahead[k], 4) >= z)(total_copy(k).wait_send)


def body(
    tokens, norm_gain, w_query, w_key, w_value, log_decay, w_conv_in, w_conv_pre,
    w_conv_post, conv_taps, w_out_ret, w_out_conv,
):
    within, bases = rotation_tables(16)
    dma = pltpu.SemaphoreType.DMA
    v = pltpu.VMEM
    scratch = [
        v((ROWS, KW), BF16), v((ROWS, KW), BF16), v((ROWS, KW), BF16),
        v((6, 2, KW, NW), BF16), v((2, 2, NW, D), BF16), v((3, ROWS, NW), F32),
        v((ROWS, NW), BF16), v((ROWS, NW), BF16), v((ROWS, NW), BF16),
        v((ROWS, NW), BF16), v((ROWS, NW), BF16), v((4, ROWS + 8, 128), F32),
        v((ROWS, NW), BF16), v((HALF, NW), BF16), v((ROWS, NW), BF16), v((HALF, NW), BF16),
        v((ROWS, NW), F32),
        v((BLOCKS, HEADS, 128, 128), BF16), v((HALF, D), F32),
        v((ROWS, 128), F32), v((128, 128), F32), v((128, 128), F32),
        v((ROWS, 128), F32), v((ROWS, 128), F32),
        v((4, 128, 128), F32), v((16, 128), F32), v((D,), BF16), v((HEADS, ROWS), F32),
        v((3, NW), BF16), v((128, 128), F32), v((128, 128), F32),
        v((BLOCKS, HEADS, 128, 128), F32), v((16, 8, 128), F32),
        v((4, 2, 128, 128), BF16), v((4, 2, 128, 128), BF16),
        v((4, 2, 128, 128), BF16), v((4, 2, 128, 128), BF16),
        v((3, 2, 128, 128), BF16), v((2, 128, 128), F32),
        v((BLOCKS, HEADS, 128, 128), F32), v((BLOCKS, HEADS, 128, 128), F32),
        v((128, 128), F32), v((128, 128), F32), v((ROWS, NW), BF16), v((HEADS, 128, 128), BF16),
        v((BLOCKS, HEADS, 128, 256), BF16),
        dma((3,)), dma((5,)), dma((12,)), dma((4,)),
    ] + [dma((3,))] * 2 + [dma((15,))] * 2 + [dma((3,))] * 8 + [dma] * 8 + [pltpu.SemaphoreType.REGULAR]
    anywhere = pl.BlockSpec(memory_space=pltpu.HBM)
    return pl.pallas_call(
        kernel,
        out_shape=pltpu.VMEM((HALF, D), BF16),
        in_specs=[anywhere] * 14,
        out_specs=pl.BlockSpec(memory_space=pltpu.VMEM),
        scratch_shapes=scratch,
        compiler_params=pltpu.CompilerParams(
            collective_id=0, has_side_effects=True, vmem_limit_bytes=56 * 1024 * 1024
        ),
    )(
        tokens, norm_gain, log_decay, conv_taps, w_key, w_value, w_query,
        w_conv_in, w_conv_pre, w_conv_post, w_out_conv, w_out_ret,
        jnp.asarray(within), jnp.asarray(bases),
    )


def solution(mesh):
    in_specs = (
        P(("fs", "sp"), "tp"),
        P(),
        P(None, "tp"),
        P(None, "tp"),
        P(None, "tp"),
        P("tp", "sp"),
        P(None, "tp"),
        P(None, "tp"),
        P(None, "tp"),
        P(None, "tp"),
        P(),
        P(),
    )
    out_specs = P(("fs", "sp", "tp"), None)
    return jax.shard_map(body, mesh=mesh, in_specs=in_specs, out_specs=out_specs, check_vma=False)
```

```python
import functools

import jax
import jax.numpy as jnp
import numpy as np
from jax import lax
from jax.experimental import pallas as pl
from jax.experimental.pallas import tpu as pltpu
from jax.sharding import PartitionSpec as P

DH = 128
SPAN = 128
ROWS = 768
HALF = 384
BLOCKS = 6
HEADS = 4
KW = 1024
NW = 512
D = 2048
EPS = 1e-06
KEY_SCALE = 128.0 ** -0.5
F32 = jnp.float32
BF16 = jnp.bfloat16
MESH = pl.DeviceIdType.MESH
WEIGHTS = ("wk", "wv", "wq", "wci", "wcp", "wcq")


def rotation_tables(places):
    half = DH // 2
    rate = 10000.0 ** (-np.arange(half, dtype=np.float64) / half)
    inner = np.arange(SPAN, dtype=np.float64)[:, None] * rate[None, :]
    inner = np.concatenate([inner, inner], axis=1)
    sign = np.concatenate([-np.ones(half), np.ones(half)])[None, :]
    within = np.stack(
        [np.cos(inner), np.sin(inner), sign * np.cos(inner), sign * np.sin(inner)]
    ).astype(np.float32)
    start = np.arange(places * BLOCKS, dtype=np.float64) * SPAN
    outer = start[:, None] * rate[None, :]
    outer = np.concatenate([outer, outer], axis=1).reshape(places, BLOCKS, DH)
    bases = np.zeros((places, 16, DH), np.float32)
    bases[:, :BLOCKS] = np.cos(outer)
    bases[:, 8 : 8 + BLOCKS] = np.sin(outer)
    return within, bases


def mm(a, b):
    return jnp.dot(a, b, preferred_element_type=F32)


def kernel(
    tok, gain, ld, taps, wk, wv, wq, wci, wcp, wcq, woc, wor, tabs, bases,
    out,
    xo, go, gp, wbuf, wob, acc, kb, vb, qb, cib, postb, gbuf, cob, cor,
    retb, retr, inside, starts, oacc, ssb, pack, pack_far, rot_c, rot_s,
    tabv, basev, gainv, ldv, tapv, ldp, cumr, colrep, lall,
    a1, a2, b1, b2, bm, pre, fade, tails, cumc, endr, qs, entry, both,
    sem_tok, sem_small, sem_w, sem_wo,
    ts, tr, ls, lr, a1s, a1r, a2s, a2r, b1s, b1r, b2s, b2r,
    hs, hr, cs, cr, rs, rr, ps, pr, met,
):
    sp = lax.axis_index("sp")
    tp = lax.axis_index("tp")
    x = lax.rem(sp, 4)
    z = lax.div(sp, 4)
    other = 1 - tp
    row_peer = [z * 4 + lax.rem(x + k, 4) for k in (1, 2, 3)]
    col_peer = [lax.rem(z + k, 4) * 4 + x for k in (1, 2, 3)]
    after = lax.rem(sp + 1, 16)
    ahead = [lax.rem(sp + k, 16) for k in range(1, 16)]
    behind = [lax.rem(sp + 16 - k, 16) for k in range(1, 16)]

    barrier = pltpu.get_barrier_semaphore()
    lall[...] = jnp.zeros_like(lall)
    a2[...] = jnp.zeros_like(a2)
    b1[...] = jnp.zeros_like(b1)
    a1[...] = jnp.zeros_like(a1)
    b2[...] = jnp.zeros_like(b2)

    @pl.when(tp == 0)
    def _():
        pl.semaphore_signal(barrier, inc=1, device_id={"tp": 1}, device_id_type=MESH)

    def remote(src, dst, send, recv, where):
        return pltpu.make_async_remote_copy(
            src_ref=src, dst_ref=dst, send_sem=send, recv_sem=recv,
            device_id=where, device_id_type=MESH,
        )

    own_k = pl.multiple_of(tp * KW, KW)
    far_k = pl.multiple_of(other * KW, KW)
    own_n = pl.multiple_of(tp * NW, NW)
    far_n = pl.multiple_of(other * NW, NW)
    own_rows = pl.ds(pl.multiple_of(tp * HALF, HALF), HALF)
    far_rows = pl.ds(pl.multiple_of(other * HALF, HALF), HALF)

    tok_load = [
        pltpu.make_async_copy(
            tok.at[pl.ds(c * 256, 256), :], xo.at[pl.ds(c * 256, 256), :], sem_tok.at[c]
        )
        for c in range(3)
    ]
    small = [
        pltpu.make_async_copy(ld, ldv, sem_small.at[0]),
        pltpu.make_async_copy(gain, gainv, sem_small.at[1]),
        pltpu.make_async_copy(taps, tapv, sem_small.at[2]),
        pltpu.make_async_copy(tabs, tabv, sem_small.at[3]),
        pltpu.make_async_copy(bases.at[sp], basev, sem_small.at[4]),
    ]
    hbm = dict(zip(WEIGHTS, (wk, wv, wq, wci, wcp, wcq)))
    index = {name: i for i, name in enumerate(WEIGHTS)}

    def w_load(name, part):
        i = index[name]
        rows = pl.ds(own_k if part == 0 else far_k, KW)
        return pltpu.make_async_copy(
            hbm[name].at[rows, :], wbuf.at[i, part], sem_w.at[i * 2 + part]
        )

    def wo_load(i, part):
        rows = pl.ds(own_n if part == 0 else far_n, NW)
        return pltpu.make_async_copy(
            (woc, wor)[i].at[rows, :], wob.at[i, part], sem_wo.at[i * 2 + part]
        )

    small[0].start()
    small[1].start()
    for copy in tok_load:
        copy.start()
    w_load("wk", 0).start()
    w_load("wv", 0).start()
    small[4].start()
    small[3].start()
    small[2].start()

    lane = lax.broadcasted_iota(jnp.int32, (SPAN, SPAN), 1)
    packed = jnp.zeros((SPAN, SPAN), F32)
    for i in range(BLOCKS):
        if i % 2 == 0:
            tok_load[i // 2].wait()
        rows = slice(i * 128, i * 128 + 128)
        value = xo[rows, :].astype(F32)
        squares = jnp.sum(value * value, axis=1, keepdims=True)
        spread = jnp.broadcast_to(squares, (SPAN, SPAN))
        ssb[rows, :] = spread
        packed = jnp.where(lane == i, spread, packed)
    pack[...] = packed

    @pl.when(tp == 1)
    def _():
        pl.semaphore_wait(barrier, 1)
        pl.semaphore_signal(met, inc=1, device_id={"tp": 0}, device_id_type=MESH)

    @pl.when(tp == 0)
    def _():
        pl.semaphore_wait(met, 1)
        for peer in ahead:
            pl.semaphore_signal(barrier, inc=1, device_id={"sp": peer}, device_id_type=MESH)

    pack_send = remote(pack, pack_far, ps, pr, {"tp": other})
    pack_send.start()
    ldp[...] = jnp.zeros_like(ldp)
    small[0].wait()
    for b in range(BLOCKS):
        ldp[b * 8 : b * 8 + HEADS, :] = ldv[:, b * SPAN : (b + 1) * SPAN]
    upper = (
        lax.broadcasted_iota(jnp.int32, (SPAN, SPAN), 0)
        <= lax.broadcasted_iota(jnp.int32, (SPAN, SPAN), 1)
    )
    ones = jnp.where(upper, 1.0, 0.0).astype(BF16)
    rest = ldp[...]
    total = jnp.zeros((SPAN, SPAN), F32)
    for _ in range(3):
        piece = rest.astype(BF16)
        total = total + mm(piece, ones)
        rest = rest - piece.astype(F32)
    cumr[...] = total
    cumc[...] = total.T
    ends = jnp.broadcast_to(total[:, SPAN - 1 : SPAN], (SPAN, SPAN))
    endr[...] = ends
    whole = ends[0:8]
    for b in range(1, BLOCKS):
        whole = whole + ends[b * 8 : b * 8 + 8]
    lall[sp] = whole

    def block_end(b, h):
        return endr[b * 8 + h : b * 8 + h + 1, :]

    def section(body):
        pl.when(sp < 16)(body)

    w_load("wq", 0).start()

    small[1].wait()
    weight = gainv[pl.ds(own_k, KW)].astype(F32).reshape(1, KW)
    pack_send.wait_recv()
    tok_send = [
        remote(
            go.at[pl.ds(c * 256, 256), :], gp.at[pl.ds(c * 256, 256), :],
            ts.at[c], tr.at[c], {"tp": other},
        )
        for c in range(3)
    ]
    for i in range(BLOCKS):
        rows = slice(i * 128, i * 128 + 128)
        level = ssb[rows, :] + jnp.broadcast_to(pack_far[:, i : i + 1], (SPAN, SPAN))
        scale = lax.rsqrt(level * (1.0 / D) + EPS)
        for c in range(KW // 128):
            at = slice(c * 128, c * 128 + 128)
            go[rows, at] = (xo[rows, at].astype(F32) * scale * weight[:, at]).astype(BF16)
        if i in (2, 4):
            tok_send[i // 2 - 1].start()
    tok_send[2].start()

    lower = (
        lax.broadcasted_iota(jnp.int32, (SPAN, SPAN), 0)
        >= lax.broadcasted_iota(jnp.int32, (SPAN, SPAN), 1)
    )

    def near_product(i):
        for n in range(2):
            cols = slice(n * 256, n * 256 + 256)
            acc[i, :, cols] = mm(go[...], wbuf[i, 0, :, cols])

    for name in ("wk", "wv", "wq"):
        w_load(name, 0).wait()
    for name in ("wk", "wv", "wq"):
        w_load(name, 1).start()
    for name in ("wci", "wcp"):
        for part in range(2):
            w_load(name, part).start()
    small[3].wait()
    small[4].wait()

    @section
    def _():
        near_product(0)
        for b in range(BLOCKS):
            rows = slice(b * 128, b * 128 + 128)
            base_c = basev[b : b + 1, :]
            base_s = basev[b + 8 : b + 9, :]
            rot_c[rows, :] = base_c * tabv[0] - base_s * tabv[1]
            rot_s[rows, :] = base_s * tabv[2] + base_c * tabv[3]
        near_product(1)
        for b in range(BLOCKS):
            for h in range(HEADS):
                i = b * 8 + h
                column = jnp.broadcast_to(cumc[:, i : i + 1], (SPAN, SPAN))
                colrep[b, h] = column
                gap = column - cumr[i : i + 1, :]
                fade[b, h] = jnp.where(lower, jnp.exp(jnp.minimum(gap, 0.0)), 0.0)
                tails[b, h] = jnp.exp(block_end(b, h) - column)
        near_product(2)

    for copy in tok_send:
        copy.wait_recv()

    def rotated(value):
        return value * rot_c[...] + pltpu.roll(value, 64, axis=1) * rot_s[...]

    exchange = []

    def key_value(n):
        cols = slice(n * 256, n * 256 + 256)
        kk = acc[0, :, cols] + mm(gp[...], wbuf[0, 1, :, cols])
        for j in range(2):
            at = slice(n * 256 + j * 128, n * 256 + j * 128 + 128)
            kb[:, at] = (rotated(kk[:, j * 128 : j * 128 + 128]) * KEY_SCALE).astype(BF16)
        vv = acc[1, :, cols] + mm(gp[...], wbuf[1, 1, :, cols])
        vb[:, cols] = vv.astype(BF16)

    def fresh_states(n):
        slot = a1.at[x] if n == 0 else b1.at[z]
        for j in range(2):
            h = n * 2 + j
            at = slice(h * 128, h * 128 + 128)
            whole = None
            for b in range(BLOCKS):
                rows = slice(b * 128, b * 128 + 128)
                weighted = (vb[rows, at].astype(F32) * tails[b, h]).astype(BF16)
                fresh = lax.dot_general(
                    kb[rows, at], weighted, (((0,), (0,)), ((), ())),
                    preferred_element_type=F32,
                )
                if b == 0:
                    whole = fresh
                else:
                    starts[b, h] = whole.astype(BF16)
                    whole = jnp.exp(block_end(b, h)) * whole + fresh
            slot[j] = whole.astype(BF16)

    def send_states(n):
        for k in range(3):
            if n == 0:
                copy = remote(a1.at[x], a1.at[x], a1s.at[k], a1r.at[k], {"sp": row_peer[k]})
            else:
                copy = remote(b1.at[z], b1.at[z], b1s.at[k], b1r.at[k], {"sp": col_peer[k]})
            pl.when((z < 3) | (x + k < 3) if n == 0 else z + k < 3)(copy.start)
            exchange.append(copy)

    for name in ("wk", "wv", "wq"):
        w_load(name, 1).wait()
    @section
    def _():
        key_value(0)
        key_value(1)

    @pl.when(tp == 0)
    def _():
        pl.semaphore_wait(barrier, 15)
        pl.semaphore_signal(met, inc=1, device_id={"tp": 1}, device_id_type=MESH)

    @pl.when(tp == 1)
    def _():
        pl.semaphore_wait(met, 1)

    def total_copy(k):
        return remote(lall.at[sp], lall.at[sp], ls.at[k], lr.at[k], {"sp": ahead[k]})

    for k in range(15):
        pl.when(lax.div(ahead[k], 4) >= z)(total_copy(k).start)

    @section
    def _():
        fresh_states(0)
        fresh_states(1)

    send_states(0)
    send_states(1)

    for name in ("wci", "wcp"):
        for part in range(2):
            w_load(name, part).wait()
    for part in range(2):
        w_load("wcq", part).start()
    for i in range(2):
        for part in range(2):
            wo_load(i, part).start()

    def full_product(i, cols):
        return (
            mm(go[...], wbuf[i, 0, :, cols]) + mm(gp[...], wbuf[i, 1, :, cols])
        ).astype(BF16)

    @section
    def _():
        for n in range(2):
            cols = slice(n * 256, n * 256 + 256)
            cib[:, cols] = full_product(3, cols)
            gated = full_product(4, cols).astype(F32) * cib[:, cols].astype(F32)
            gated = gated.astype(BF16).astype(F32)
            for j in range(2):
                gbuf[n * 2 + j, 8 : 8 + ROWS, :] = gated[:, j * 128 : j * 128 + 128]

    halo = remote(
        gbuf.at[:, pl.ds(ROWS, 8), :], gbuf.at[:, pl.ds(0, 8), :], hs, hr, {"sp": after}
    )
    pl.when(sp < 15)(halo.start)

    for k in range(15):
        pl.when(lax.div(behind[k], 4) <= z)(total_copy(k).wait_recv)
    totals = [[lall[4 * i + j] for j in range(4)] for i in range(4)]
    line = [lall[4 * z + j] for j in range(4)]

    def between(low, high):
        parts = [
            jnp.where(jnp.logical_and(i > low, i < high), line[i], 0.0) for i in range(4)
        ]
        return (parts[0] + parts[1]) + (parts[2] + parts[3])

    row_sums = [(t[0] + t[1]) + (t[2] + t[3]) for t in totals]
    suffix = []
    for t in totals:
        parts = [jnp.where(j > x, t[j], 0.0) for j in range(4)]
        suffix.append((parts[0] + parts[1]) + (parts[2] + parts[3]))
    before_me = between(-1, x)

    def rows_between(low):
        parts = [
            jnp.where(jnp.logical_and(i > low, i < z), row_sums[i], 0.0) for i in range(4)
        ]
        return (parts[0] + parts[1]) + (parts[2] + parts[3])

    def lane_row(weight, h):
        return weight[h : h + 1, :]

    second = []
    above = [
        jnp.where(i < z, jnp.exp(suffix[i] + rows_between(i)), 0.0) for i in range(4)
    ]
    for k in range(3):
        pl.when(z > k)(exchange[3 + k].wait_recv)
    e_own = jnp.exp(before_me)
    for j in range(2):
        h = 2 + j
        column = lane_row(above[0], h) * b1[0, j].astype(F32)
        for i in range(1, 4):
            column = column + lane_row(above[i], h) * b1[i, j].astype(F32)
        mine = b1[z, j].astype(F32)
        b2[x, j] = (lane_row(e_own, h) * column).astype(BF16)
        for k in range(3):
            target = lax.rem(x + k + 1, 4)
            e_col = jnp.exp(between(-1, target))
            e_mine = jnp.where(x < target, jnp.exp(between(x, target)), 0.0)
            bm[k, j] = (lane_row(e_col, h) * column + lane_row(e_mine, h) * mine).astype(BF16)
    for k in range(3):
        copy = remote(bm.at[k], b2.at[x], b2s.at[k], b2r.at[k], {"sp": row_peer[k]})
        pl.when((z > 0) | (x + k < 3))(copy.start)
        second.append(copy)

    for part in range(2):
        w_load("wcq", part).wait()
    @section
    def _():
        for n in range(2):
            cols = slice(n * 256, n * 256 + 256)
            postb[:, cols] = full_product(5, cols)


    second += [
        remote(a2.at[z], a2.at[z], a2s.at[k], a2r.at[k], {"sp": col_peer[k]})
        for k in range(3)
    ]

    def pass_rows():
        to_end = [jnp.exp(between(i, 4)) for i in range(4)]
        to_me = [jnp.where(i < x, jnp.exp(between(i, x)), 0.0) for i in range(4)]
        for k in range(3):
            pl.when((z < 3) | (x > k))(exchange[k].wait_recv)
        for j in range(2):
            parts = [a1[i, j].astype(F32) for i in range(4)]
            row_state = lane_row(to_end[0], j) * parts[0]
            prefix = lane_row(to_me[0], j) * parts[0]
            for i in range(1, 4):
                row_state = row_state + lane_row(to_end[i], j) * parts[i]
                prefix = prefix + lane_row(to_me[i], j) * parts[i]
            pre[j] = prefix
            a2[z, j] = row_state.astype(BF16)
        for k in range(3):
            pl.when(z + k < 3)(second[3 + k].start)

    pl.when(x > 0)(pass_rows)

    @section
    def _():
        for n in range(2):
            cols = slice(n * 256, n * 256 + 256)
            qq = acc[2, :, cols] + mm(gp[...], wbuf[2, 1, :, cols])
            for j in range(2):
                at = slice(n * 256 + j * 128, n * 256 + j * 128 + 128)
                qb[:, at] = rotated(qq[:, j * 128 : j * 128 + 128]).astype(BF16)

    pl.when(x == 0)(pass_rows)

    small[2].wait()
    pl.when(sp > 0)(halo.wait_recv)

    @pl.when(sp == 0)
    def _():
        gbuf[:, 0:8, :] = jnp.zeros((4, 8, 128), F32)

    @section
    def _():
        for c in range(4):
            at = slice(c * 128, c * 128 + 128)
            summed = jnp.zeros((ROWS, 128), F32)
            for i in range(3):
                summed = summed + tapv[i : i + 1, at].astype(F32) * gbuf[c, 6 + i : 6 + i + ROWS, :]
            cob[:, at] = (postb[:, at].astype(F32) * summed).astype(BF16)

    conv_send = remote(cob.at[far_rows, :], cor, cs, cr, {"tp": other})
    conv_send.start()

    for i in range(2):
        for part in range(2):
            wo_load(i, part).wait()

    def score_block(b):
        rows = slice(b * 128, b * 128 + 128)
        for h in range(HEADS):
            at = slice(h * 128, h * 128 + 128)
            scores = lax.dot_general(
                qb[rows, at], kb[rows, at], (((1,), (1,)), ((), ())),
                preferred_element_type=F32,
            )
            both[b, h, :, :128] = (scores * fade[b, h]).astype(BF16)
            query = qb[rows, at].astype(F32)
            if b == 0:
                qs[rows, at] = (query * jnp.exp(colrep[b, h])).astype(BF16)
            else:
                both[b, h, :, 128:] = (query * jnp.exp(colrep[b, h])).astype(BF16)
                offset = endr[h : h + 1, :]
                for e in range(1, b):
                    offset = offset + block_end(e, h)
                qs[rows, at] = (query * jnp.exp(colrep[b, h] + offset)).astype(BF16)

    def value_block(b):
        rows = slice(b * 128, b * 128 + 128)
        for h in range(HEADS):
            at = slice(h * 128, h * 128 + 128)
            if b == 0:
                inside[rows, at] = mm(both[b, h, :, :128], vb[rows, at])
            else:
                inside[rows, at] = mm(
                    both[b, h],
                    jnp.concatenate([vb[rows, at], starts[b, h]], axis=0),
                )

    @section
    def _():
        for n in range(8):
            cols = slice(n * 256, n * 256 + 256)
            oacc[:, cols] = mm(cob[own_rows, :], wob[0, 0, :, cols])
            if n < 6:
                score_block(n)
            if n >= 2:
                value_block(n - 2)

    conv_send.wait_recv()

    for k in range(3):
        pl.when((z > 0) | (x > k))(second[k].wait_recv)
        pl.when(z > k)(second[3 + k].wait_recv)
    down = [
        jnp.where(i < z, jnp.exp(rows_between(i) + before_me), 0.0) for i in range(4)
    ]
    for h in range(HEADS):
        j = h % 2
        if h < 2:
            state = pre[j]
            for i in range(4):
                state = state + lane_row(down[i], h) * a2[i, j].astype(F32)
        else:
            state = b2[0, j].astype(F32)
            for i in range(1, 4):
                state = state + b2[i, j].astype(F32)
        entry[h] = state.astype(BF16)

    def across(first, i):
        rows = pl.ds(pl.multiple_of(first + i * 128, 128), 128)
        for h in range(HEADS):
            at = slice(h * 128, h * 128 + 128)
            value = inside[rows, at] + mm(qs[rows, at], entry[h])
            level = jnp.mean(value * value, axis=1, keepdims=True)
            retb[rows, at] = (value * lax.rsqrt(level + EPS)).astype(BF16)

    @section
    def _():
        for i in range(3):
            across(other * HALF, i)

    ret_send = remote(retb.at[far_rows, :], retr, rs, rr, {"tp": other})
    ret_send.start()

    @section
    def _():
        for n in range(8):
            cols = slice(n * 256, n * 256 + 256)
            oacc[:, cols] += mm(cor[...], wob[0, 1, :, cols])
            if n < 3:
                across(tp * HALF, n)


    @section
    def _():
        for n in range(8):
            cols = slice(n * 256, n * 256 + 256)
            oacc[:, cols] += mm(retb[own_rows, :], wob[1, 0, :, cols])

    ret_send.wait_recv()

    @section
    def _():
        for n in range(8):
            cols = slice(n * 256, n * 256 + 256)
            out[:, cols] = (oacc[:, cols] + mm(retr[...], wob[1, 1, :, cols])).astype(BF16)

    for copy in [pack_send, conv_send, ret_send] + tok_send:
        copy.wait_send()
    pl.when(sp < 15)(halo.wait_send)
    for k in range(3):
        pl.when((z < 3) | (x + k < 3))(exchange[k].wait_send)
        pl.when((z > 0) | (x + k < 3))(second[k].wait_send)
        pl.when(z + k < 3)(exchange[3 + k].wait_send)
        pl.when(z + k < 3)(second[3 + k].wait_send)
    for k in range(15):
        pl.when(lax.div(ahead[k], 4) >= z)(total_copy(k).wait_send)


def body(
    tokens, norm_gain, w_query, w_key, w_value, log_decay, w_conv_in, w_conv_pre,
    w_conv_post, conv_taps, w_out_ret, w_out_conv,
):
    within, bases = rotation_tables(16)
    dma = pltpu.SemaphoreType.DMA
    v = pltpu.VMEM
    scratch = [
        v((ROWS, KW), BF16), v((ROWS, KW), BF16), v((ROWS, KW), BF16),
        v((6, 2, KW, NW), BF16), v((2, 2, NW, D), BF16), v((3, ROWS, NW), F32),
        v((ROWS, NW), BF16), v((ROWS, NW), BF16), v((ROWS, NW), BF16),
        v((ROWS, NW), BF16), v((ROWS, NW), BF16), v((4, ROWS + 8, 128), F32),
        v((ROWS, NW), BF16), v((HALF, NW), BF16), v((ROWS, NW), BF16), v((HALF, NW), BF16),
        v((ROWS, NW), F32),
        v((BLOCKS, HEADS, 128, 128), BF16), v((HALF, D), F32),
        v((ROWS, 128), F32), v((128, 128), F32), v((128, 128), F32),
        v((ROWS, 128), F32), v((ROWS, 128), F32),
        v((4, 128, 128), F32), v((16, 128), F32), v((D,), BF16), v((HEADS, ROWS), F32),
        v((3, NW), BF16), v((128, 128), F32), v((128, 128), F32),
        v((BLOCKS, HEADS, 128, 128), F32), v((16, 8, 128), F32),
        v((4, 2, 128, 128), BF16), v((4, 2, 128, 128), BF16),
        v((4, 2, 128, 128), BF16), v((4, 2, 128, 128), BF16),
        v((3, 2, 128, 128), BF16), v((2, 128, 128), F32),
        v((BLOCKS, HEADS, 128, 128), F32), v((BLOCKS, HEADS, 128, 128), F32),
        v((128, 128), F32), v((128, 128), F32), v((ROWS, NW), BF16), v((HEADS, 128, 128), BF16),
        v((BLOCKS, HEADS, 128, 256), BF16),
        dma((3,)), dma((5,)), dma((12,)), dma((4,)),
    ] + [dma((3,))] * 2 + [dma((15,))] * 2 + [dma((3,))] * 8 + [dma] * 8 + [pltpu.SemaphoreType.REGULAR]
    anywhere = pl.BlockSpec(memory_space=pltpu.HBM)
    return pl.pallas_call(
        kernel,
        out_shape=pltpu.VMEM((HALF, D), BF16),
        in_specs=[anywhere] * 14,
        out_specs=pl.BlockSpec(memory_space=pltpu.VMEM),
        scratch_shapes=scratch,
        compiler_params=pltpu.CompilerParams(
            collective_id=0, has_side_effects=True, vmem_limit_bytes=56 * 1024 * 1024
        ),
    )(
        tokens, norm_gain, log_decay, conv_taps, w_key, w_value, w_query,
        w_conv_in, w_conv_pre, w_conv_post, w_out_conv, w_out_ret,
        jnp.asarray(within), jnp.asarray(bases),
    )


def solution(mesh):
    in_specs = (
        P(("fs", "sp"), "tp"),
        P(),
        P(None, "tp"),
        P(None, "tp"),
        P(None, "tp"),
        P("tp", "sp"),
        P(None, "tp"),
        P(None, "tp"),
        P(None, "tp"),
        P(None, "tp"),
        P(),
        P(),
    )
    out_specs = P(("fs", "sp", "tp"), None)
    return jax.shard_map(body, mesh=mesh, in_specs=in_specs, out_specs=out_specs, check_vma=False)
```

```python
import functools

import jax
import jax.numpy as jnp
import numpy as np
from jax import lax
from jax.experimental import pallas as pl
from jax.experimental.pallas import tpu as pltpu
from jax.sharding import PartitionSpec as P

DH = 128
SPAN = 128
ROWS = 768
HALF = 384
BLOCKS = 6
HEADS = 4
KW = 1024
NW = 512
D = 2048
EPS = 1e-06
KEY_SCALE = 128.0 ** -0.5
F32 = jnp.float32
BF16 = jnp.bfloat16
MESH = pl.DeviceIdType.MESH
WEIGHTS = ("wk", "wv", "wq", "wci", "wcp", "wcq")


def rotation_tables(places):
    half = DH // 2
    rate = 10000.0 ** (-np.arange(half, dtype=np.float64) / half)
    inner = np.arange(SPAN, dtype=np.float64)[:, None] * rate[None, :]
    inner = np.concatenate([inner, inner], axis=1)
    sign = np.concatenate([-np.ones(half), np.ones(half)])[None, :]
    within = np.stack(
        [np.cos(inner), np.sin(inner), sign * np.cos(inner), sign * np.sin(inner)]
    ).astype(np.float32)
    start = np.arange(places * BLOCKS, dtype=np.float64) * SPAN
    outer = start[:, None] * rate[None, :]
    outer = np.concatenate([outer, outer], axis=1).reshape(places, BLOCKS, DH)
    bases = np.zeros((places, 16, DH), np.float32)
    bases[:, :BLOCKS] = np.cos(outer)
    bases[:, 8 : 8 + BLOCKS] = np.sin(outer)
    return within, bases


def mm(a, b):
    return jnp.dot(a, b, preferred_element_type=F32)


def kernel(
    tok, gain, ld, taps, wk, wv, wq, wci, wcp, wcq, woc, wor, tabs, bases,
    out,
    xo, go, gp, wbuf, wob, acc, kb, vb, qb, cib, postb, gbuf, cob, cor,
    retb, retr, inside, starts, oacc, ssb, pack, pack_far, rot_c, rot_s,
    tabv, basev, gainv, ldv, tapv, ldp, cumr, colrep, lall,
    a1, a2, b1, b2, bm, pre, fade, tails, cumc, endr, qs, entry, both, downv,
    sem_tok, sem_small, sem_w, sem_wo,
    ts, tr, ls, lr, a1s, a1r, a2s, a2r, b1s, b1r, b2s, b2r,
    hs, hr, cs, cr, rs, rr, ps, pr, met,
):
    sp = lax.axis_index("sp")
    tp = lax.axis_index("tp")
    x = lax.rem(sp, 4)
    z = lax.div(sp, 4)
    other = 1 - tp
    row_peer = [z * 4 + lax.rem(x + k, 4) for k in (1, 2, 3)]
    col_peer = [lax.rem(z + k, 4) * 4 + x for k in (1, 2, 3)]
    after = lax.rem(sp + 1, 16)
    ahead = [lax.rem(sp + k, 16) for k in range(1, 16)]
    behind = [lax.rem(sp + 16 - k, 16) for k in range(1, 16)]

    def remote(src, dst, send, recv, where):
        return pltpu.make_async_remote_copy(
            src_ref=src, dst_ref=dst, send_sem=send, recv_sem=recv,
            device_id=where, device_id_type=MESH,
        )

    own_k = pl.multiple_of(tp * KW, KW)
    far_k = pl.multiple_of(other * KW, KW)
    own_n = pl.multiple_of(tp * NW, NW)
    far_n = pl.multiple_of(other * NW, NW)
    own_rows = pl.ds(pl.multiple_of(tp * HALF, HALF), HALF)
    far_rows = pl.ds(pl.multiple_of(other * HALF, HALF), HALF)

    tok_load = [
        pltpu.make_async_copy(
            tok.at[pl.ds(c * 256, 256), :], xo.at[pl.ds(c * 256, 256), :], sem_tok.at[c]
        )
        for c in range(3)
    ]
    small = [
        pltpu.make_async_copy(ld, ldv, sem_small.at[0]),
        pltpu.make_async_copy(gain, gainv, sem_small.at[1]),
        pltpu.make_async_copy(taps, tapv, sem_small.at[2]),
        pltpu.make_async_copy(tabs, tabv, sem_small.at[3]),
        pltpu.make_async_copy(bases.at[sp], basev, sem_small.at[4]),
    ]
    hbm = dict(zip(WEIGHTS, (wk, wv, wq, wci, wcp, wcq)))
    index = {name: i for i, name in enumerate(WEIGHTS)}

    def w_load(name, part):
        i = index[name]
        rows = pl.ds(own_k if part == 0 else far_k, KW)
        return pltpu.make_async_copy(
            hbm[name].at[rows, :], wbuf.at[i, part], sem_w.at[i * 2 + part]
        )

    def wo_load(i, part):
        rows = pl.ds(own_n if part == 0 else far_n, NW)
        return pltpu.make_async_copy(
            (woc, wor)[i].at[rows, :], wob.at[i, part], sem_wo.at[i * 2 + part]
        )

    for copy in tok_load:
        copy.start()
    small[0].start()
    small[1].start()
    w_load("wk", 0).start()
    w_load("wv", 0).start()
    small[4].start()
    small[3].start()
    small[2].start()

    barrier = pltpu.get_barrier_semaphore()
    lall[...] = jnp.zeros_like(lall)
    a2[...] = jnp.zeros_like(a2)
    b1[...] = jnp.zeros_like(b1)
    a1[...] = jnp.zeros_like(a1)
    b2[...] = jnp.zeros_like(b2)

    @pl.when(tp == 0)
    def _():
        pl.semaphore_signal(barrier, inc=1, device_id={"tp": 1}, device_id_type=MESH)

    @pl.when(tp == 1)
    def _():
        pl.semaphore_wait(barrier, 1)
        pl.semaphore_signal(met, inc=1, device_id={"tp": 0}, device_id_type=MESH)

    @pl.when(tp == 0)
    def _():
        pl.semaphore_wait(met, 1)
        for peer in ahead:
            pl.semaphore_signal(barrier, inc=1, device_id={"sp": peer}, device_id_type=MESH)

    lane = lax.broadcasted_iota(jnp.int32, (SPAN, SPAN), 1)
    packed = jnp.zeros((SPAN, SPAN), F32)
    for i in range(BLOCKS):
        if i % 2 == 0:
            tok_load[i // 2].wait()
        rows = slice(i * 128, i * 128 + 128)
        value = xo[rows, :].astype(F32)
        squares = jnp.sum(value * value, axis=1, keepdims=True)
        spread = jnp.broadcast_to(squares, (SPAN, SPAN))
        ssb[rows, :] = spread
        packed = jnp.where(lane == i, spread, packed)
    pack[...] = packed

    pack_send = remote(pack, pack_far, ps, pr, {"tp": other})
    pack_send.start()
    ldp[...] = jnp.zeros_like(ldp)
    small[0].wait()
    for b in range(BLOCKS):
        ldp[b * 8 : b * 8 + HEADS, :] = ldv[:, b * SPAN : (b + 1) * SPAN]
    upper = (
        lax.broadcasted_iota(jnp.int32, (SPAN, SPAN), 0)
        <= lax.broadcasted_iota(jnp.int32, (SPAN, SPAN), 1)
    )
    ones = jnp.where(upper, 1.0, 0.0).astype(BF16)
    rest = ldp[...]
    total = jnp.zeros((SPAN, SPAN), F32)
    for _ in range(3):
        piece = rest.astype(BF16)
        total = total + mm(piece, ones)
        rest = rest - piece.astype(F32)
    cumr[...] = total
    cumc[...] = total.T
    ends = jnp.broadcast_to(total[:, SPAN - 1 : SPAN], (SPAN, SPAN))
    endr[...] = ends
    whole = ends[0:8]
    for b in range(1, BLOCKS):
        whole = whole + ends[b * 8 : b * 8 + 8]
    lall[sp] = whole

    def block_end(b, h):
        return endr[b * 8 + h : b * 8 + h + 1, :]

    def section(body):
        pl.when(sp < 16)(body)

    w_load("wq", 0).start()

    small[1].wait()
    weight = gainv[pl.ds(own_k, KW)].astype(F32).reshape(1, KW)
    pack_send.wait_recv()
    tok_send = [
        remote(
            go.at[pl.ds(c * 256, 256), :], gp.at[pl.ds(c * 256, 256), :],
            ts.at[c], tr.at[c], {"tp": other},
        )
        for c in range(3)
    ]
    for i in range(BLOCKS):
        rows = slice(i * 128, i * 128 + 128)
        level = ssb[rows, :] + jnp.broadcast_to(pack_far[:, i : i + 1], (SPAN, SPAN))
        scale = lax.rsqrt(level * (1.0 / D) + EPS)
        for c in range(KW // 128):
            at = slice(c * 128, c * 128 + 128)
            go[rows, at] = (xo[rows, at].astype(F32) * scale * weight[:, at]).astype(BF16)
        if i in (2, 4):
            tok_send[i // 2 - 1].start()
    tok_send[2].start()

    lower = (
        lax.broadcasted_iota(jnp.int32, (SPAN, SPAN), 0)
        >= lax.broadcasted_iota(jnp.int32, (SPAN, SPAN), 1)
    )

    def near_product(i):
        for n in range(2):
            cols = slice(n * 256, n * 256 + 256)
            acc[i, :, cols] = mm(go[...], wbuf[i, 0, :, cols])

    for name in ("wk", "wv", "wq"):
        w_load(name, 0).wait()
    for name in ("wk", "wv", "wq"):
        w_load(name, 1).start()
    for name in ("wci", "wcp"):
        for part in range(2):
            w_load(name, part).start()
    small[3].wait()
    small[4].wait()

    @section
    def _():
        near_product(0)
        for b in range(BLOCKS):
            rows = slice(b * 128, b * 128 + 128)
            base_c = basev[b : b + 1, :]
            base_s = basev[b + 8 : b + 9, :]
            rot_c[rows, :] = base_c * tabv[0] - base_s * tabv[1]
            rot_s[rows, :] = base_s * tabv[2] + base_c * tabv[3]
        near_product(1)
        for b in range(BLOCKS):
            for h in range(HEADS):
                i = b * 8 + h
                column = jnp.broadcast_to(cumc[:, i : i + 1], (SPAN, SPAN))
                colrep[b, h] = column
                gap = column - cumr[i : i + 1, :]
                fade[b, h] = jnp.where(lower, jnp.exp(jnp.minimum(gap, 0.0)), 0.0)
                tails[b, h] = jnp.exp(block_end(b, h) - column)
        near_product(2)

    for copy in tok_send:
        copy.wait_recv()

    def rotated(value):
        return value * rot_c[...] + pltpu.roll(value, 64, axis=1) * rot_s[...]

    exchange = []

    def keys_of(n):
        cols = slice(n * 256, n * 256 + 256)
        kk = acc[0, :, cols] + mm(gp[...], wbuf[0, 1, :, cols])
        for j in range(2):
            at = slice(n * 256 + j * 128, n * 256 + j * 128 + 128)
            kb[:, at] = (rotated(kk[:, j * 128 : j * 128 + 128]) * KEY_SCALE).astype(BF16)

    def values_of(n):
        cols = slice(n * 256, n * 256 + 256)
        vv = acc[1, :, cols] + mm(gp[...], wbuf[1, 1, :, cols])
        vb[:, cols] = vv.astype(BF16)

    def fresh_states(n):
        slot = a1.at[x] if n == 0 else b1.at[z]
        for j in range(2):
            h = n * 2 + j
            at = slice(h * 128, h * 128 + 128)
            whole = None
            for b in range(BLOCKS):
                rows = slice(b * 128, b * 128 + 128)
                weighted = (vb[rows, at].astype(F32) * tails[b, h]).astype(BF16)
                fresh = lax.dot_general(
                    kb[rows, at], weighted, (((0,), (0,)), ((), ())),
                    preferred_element_type=F32,
                )
                if b == 0:
                    whole = fresh
                else:
                    starts[b, h] = whole.astype(BF16)
                    whole = jnp.exp(block_end(b, h)) * whole + fresh
            slot[j] = whole.astype(BF16)

    def start_along_row(copies, always):
        pl.when((x == 2) & always)(copies[1].start)
        for k in range(3):
            wanted = always | (x + k < 3)
            pl.when(wanted & (x != 2) if k == 1 else wanted)(copies[k].start)

    def send_states(n):
        for k in range(3):
            if n == 0:
                copy = remote(a1.at[x], a1.at[x], a1s.at[k], a1r.at[k], {"sp": row_peer[k]})
            else:
                copy = remote(b1.at[z], b1.at[z], b1s.at[k], b1r.at[k], {"sp": col_peer[k]})
            exchange.append(copy)
            if n == 1:
                pl.when(z + k < 3)(copy.start)
        if n == 0:
            start_along_row(exchange, z < 3)

    for name in ("wk", "wv", "wq"):
        w_load(name, 1).wait()
    @pl.when(tp == 0)
    def _():
        pl.semaphore_wait(barrier, 15)
        pl.semaphore_signal(met, inc=1, device_id={"tp": 1}, device_id_type=MESH)

    @pl.when(tp == 1)
    def _():
        pl.semaphore_wait(met, 1)

    def total_copy(k):
        return remote(lall.at[sp], lall.at[sp], ls.at[k], lr.at[k], {"sp": ahead[k]})

    for k in range(15):
        pl.when(lax.div(ahead[k], 4) >= z)(total_copy(k).start)

    @section
    def _():
        keys_of(0)
        keys_of(1)
        values_of(0)
        values_of(1)

    @section
    def _():
        fresh_states(0)
        fresh_states(1)

    send_states(0)
    send_states(1)

    for name in ("wci", "wcp"):
        for part in range(2):
            w_load(name, part).wait()
    for part in range(2):
        w_load("wcq", part).start()
    for i in range(2):
        for part in range(2):
            wo_load(i, part).start()

    def full_product(i, cols):
        return (
            mm(go[...], wbuf[i, 0, :, cols]) + mm(gp[...], wbuf[i, 1, :, cols])
        ).astype(BF16)

    @section
    def _():
        for n in range(2):
            cols = slice(n * 256, n * 256 + 256)
            cib[:, cols] = full_product(3, cols)
            gated = full_product(4, cols).astype(F32) * cib[:, cols].astype(F32)
            gated = gated.astype(BF16).astype(F32)
            for j in range(2):
                gbuf[n * 2 + j, 8 : 8 + ROWS, :] = gated[:, j * 128 : j * 128 + 128]

    halo = remote(
        gbuf.at[:, pl.ds(ROWS, 8), :], gbuf.at[:, pl.ds(0, 8), :], hs, hr, {"sp": after}
    )
    pl.when(sp < 15)(halo.start)

    for k in range(15):
        pl.when(lax.div(behind[k], 4) <= z)(total_copy(k).wait_recv)
    totals = [[lall[4 * i + j] for j in range(4)] for i in range(4)]
    line = [lall[4 * z + j] for j in range(4)]

    def between(low, high):
        parts = [
            jnp.where(jnp.logical_and(i > low, i < high), line[i], 0.0) for i in range(4)
        ]
        return (parts[0] + parts[1]) + (parts[2] + parts[3])

    row_sums = [(t[0] + t[1]) + (t[2] + t[3]) for t in totals]
    suffix = []
    for t in totals:
        parts = [jnp.where(j > x, t[j], 0.0) for j in range(4)]
        suffix.append((parts[0] + parts[1]) + (parts[2] + parts[3]))
    before_me = between(-1, x)

    def rows_between(low):
        parts = [
            jnp.where(jnp.logical_and(i > low, i < z), row_sums[i], 0.0) for i in range(4)
        ]
        return (parts[0] + parts[1]) + (parts[2] + parts[3])

    def lane_row(weight, h):
        return weight[h : h + 1, :]

    second = []
    above = [
        jnp.where(i < z, jnp.exp(suffix[i] + rows_between(i)), 0.0) for i in range(4)
    ]
    for k in range(3):
        pl.when(z > k)(exchange[3 + k].wait_recv)
    e_own = jnp.exp(before_me)
    for j in range(2):
        h = 2 + j
        column = lane_row(above[0], h) * b1[0, j].astype(F32)
        for i in range(1, 4):
            column = column + lane_row(above[i], h) * b1[i, j].astype(F32)
        mine = b1[z, j].astype(F32)
        b2[x, j] = (lane_row(e_own, h) * column).astype(BF16)
        for k in range(3):
            target = lax.rem(x + k + 1, 4)
            e_col = jnp.exp(between(-1, target))
            e_mine = jnp.where(x < target, jnp.exp(between(x, target)), 0.0)
            bm[k, j] = (lane_row(e_col, h) * column + lane_row(e_mine, h) * mine).astype(BF16)
    for k in range(3):
        copy = remote(bm.at[k], b2.at[x], b2s.at[k], b2r.at[k], {"sp": row_peer[k]})
        second.append(copy)
    start_along_row(second, z > 0)

    for part in range(2):
        w_load("wcq", part).wait()
    @section
    def _():
        for n in range(2):
            cols = slice(n * 256, n * 256 + 256)
            qq = acc[2, :, cols] + mm(gp[...], wbuf[2, 1, :, cols])
            for j in range(2):
                at = slice(n * 256 + j * 128, n * 256 + j * 128 + 128)
                qb[:, at] = rotated(qq[:, j * 128 : j * 128 + 128]).astype(BF16)
        postb[:, 0:256] = full_product(5, slice(0, 256))


    second += [
        remote(a2.at[z], a2.at[z], a2s.at[k], a2r.at[k], {"sp": col_peer[k]})
        for k in range(3)
    ]

    def pass_rows():
        to_end = [jnp.exp(between(i, 4)) for i in range(4)]
        to_me = [jnp.where(i < x, jnp.exp(between(i, x)), 0.0) for i in range(4)]
        for k in range(3):
            pl.when((z < 3) | (x > k))(exchange[k].wait_recv)
        for j in range(2):
            parts = [a1[i, j].astype(F32) for i in range(4)]
            row_state = lane_row(to_end[0], j) * parts[0]
            prefix = lane_row(to_me[0], j) * parts[0]
            for i in range(1, 4):
                row_state = row_state + lane_row(to_end[i], j) * parts[i]
                prefix = prefix + lane_row(to_me[i], j) * parts[i]
            pre[j] = prefix
            a2[z, j] = row_state.astype(BF16)
        for k in range(3):
            pl.when(z + k < 3)(second[3 + k].start)

    pl.when(x > 0)(pass_rows)

    @section
    def _():
        postb[:, 256:512] = full_product(5, slice(256, 512))

    pl.when(x == 0)(pass_rows)
    for i in range(4):
        downv[i] = jnp.where(i < z, jnp.exp(rows_between(i) + before_me), 0.0)

    small[2].wait()
    pl.when(sp > 0)(halo.wait_recv)

    @pl.when(sp == 0)
    def _():
        gbuf[:, 0:8, :] = jnp.zeros((4, 8, 128), F32)

    @section
    def _():
        for c in range(4):
            at = slice(c * 128, c * 128 + 128)
            summed = jnp.zeros((ROWS, 128), F32)
            for i in range(3):
                summed = summed + tapv[i : i + 1, at].astype(F32) * gbuf[c, 6 + i : 6 + i + ROWS, :]
            cob[:, at] = (postb[:, at].astype(F32) * summed).astype(BF16)

    conv_send = remote(cob.at[far_rows, :], cor, cs, cr, {"tp": other})
    conv_send.start()

    for i in range(2):
        for part in range(2):
            wo_load(i, part).wait()

    def score_block(b):
        rows = slice(b * 128, b * 128 + 128)
        for h in range(HEADS):
            at = slice(h * 128, h * 128 + 128)
            scores = lax.dot_general(
                qb[rows, at], kb[rows, at], (((1,), (1,)), ((), ())),
                preferred_element_type=F32,
            )
            both[b, h, :, :128] = (scores * fade[b, h]).astype(BF16)
            query = qb[rows, at].astype(F32)
            if b == 0:
                qs[rows, at] = (query * jnp.exp(colrep[b, h])).astype(BF16)
            else:
                both[b, h, :, 128:] = (query * jnp.exp(colrep[b, h])).astype(BF16)
                offset = endr[h : h + 1, :]
                for e in range(1, b):
                    offset = offset + block_end(e, h)
                qs[rows, at] = (query * jnp.exp(colrep[b, h] + offset)).astype(BF16)

    def value_block(b):
        rows = slice(b * 128, b * 128 + 128)
        for h in range(HEADS):
            at = slice(h * 128, h * 128 + 128)
            if b == 0:
                inside[rows, at] = mm(both[b, h, :, :128], vb[rows, at])
            else:
                inside[rows, at] = mm(
                    both[b, h],
                    jnp.concatenate([vb[rows, at], starts[b, h]], axis=0),
                )

    @section
    def _():
        for n in range(8):
            cols = slice(n * 256, n * 256 + 256)
            oacc[:, cols] = mm(cob[own_rows, :], wob[0, 0, :, cols])
            if n < 6:
                score_block(n)
            if n >= 2:
                value_block(n - 2)

    conv_send.wait_recv()

    for k in range(15):
        pl.when(lax.div(ahead[k], 4) >= z)(total_copy(k).wait_send)
    for k in range(3):
        pl.when((z < 3) | (x + k < 3))(exchange[k].wait_send)
        pl.when(z + k < 3)(exchange[3 + k].wait_send)
    pl.when(sp < 15)(halo.wait_send)
    for copy in [pack_send] + tok_send:
        copy.wait_send()
    for k in range(3):
        pl.when((z > 0) | (x > k))(second[k].wait_recv)
        pl.when(z > k)(second[3 + k].wait_recv)
    down = [downv[i] for i in range(4)]
    for h in range(HEADS):
        j = h % 2
        if h < 2:
            state = pre[j]
            for i in range(4):
                state = state + lane_row(down[i], h) * a2[i, j].astype(F32)
        else:
            state = b2[0, j].astype(F32)
            for i in range(1, 4):
                state = state + b2[i, j].astype(F32)
        entry[h] = state.astype(BF16)

    def across(first, i):
        rows = pl.ds(pl.multiple_of(first + i * 128, 128), 128)
        for h in range(HEADS):
            at = slice(h * 128, h * 128 + 128)
            value = inside[rows, at] + mm(qs[rows, at], entry[h])
            level = jnp.mean(value * value, axis=1, keepdims=True)
            retb[rows, at] = (value * lax.rsqrt(level + EPS)).astype(BF16)

    @section
    def _():
        for i in range(3):
            across(other * HALF, i)

    ret_send = remote(retb.at[far_rows, :], retr, rs, rr, {"tp": other})
    ret_send.start()

    @section
    def _():
        for n in range(8):
            cols = slice(n * 256, n * 256 + 256)
            oacc[:, cols] += mm(cor[...], wob[0, 1, :, cols])
            if n < 3:
                across(tp * HALF, n)


    @section
    def _():
        for n in range(8):
            cols = slice(n * 256, n * 256 + 256)
            oacc[:, cols] += mm(retb[own_rows, :], wob[1, 0, :, cols])

    ret_send.wait_recv()

    @section
    def _():
        for n in range(8):
            cols = slice(n * 256, n * 256 + 256)
            out[:, cols] = (oacc[:, cols] + mm(retr[...], wob[1, 1, :, cols])).astype(BF16)

    for copy in [conv_send, ret_send]:
        copy.wait_send()
    for k in range(3):
        pl.when((z > 0) | (x + k < 3))(second[k].wait_send)
        pl.when(z + k < 3)(second[3 + k].wait_send)


def body(
    tokens, norm_gain, w_query, w_key, w_value, log_decay, w_conv_in, w_conv_pre,
    w_conv_post, conv_taps, w_out_ret, w_out_conv,
):
    within, bases = rotation_tables(16)
    dma = pltpu.SemaphoreType.DMA
    v = pltpu.VMEM
    scratch = [
        v((ROWS, KW), BF16), v((ROWS, KW), BF16), v((ROWS, KW), BF16),
        v((6, 2, KW, NW), BF16), v((2, 2, NW, D), BF16), v((3, ROWS, NW), F32),
        v((ROWS, NW), BF16), v((ROWS, NW), BF16), v((ROWS, NW), BF16),
        v((ROWS, NW), BF16), v((ROWS, NW), BF16), v((4, ROWS + 8, 128), F32),
        v((ROWS, NW), BF16), v((HALF, NW), BF16), v((ROWS, NW), BF16), v((HALF, NW), BF16),
        v((ROWS, NW), F32),
        v((BLOCKS, HEADS, 128, 128), BF16), v((HALF, D), F32),
        v((ROWS, 128), F32), v((128, 128), F32), v((128, 128), F32),
        v((ROWS, 128), F32), v((ROWS, 128), F32),
        v((4, 128, 128), F32), v((16, 128), F32), v((D,), BF16), v((HEADS, ROWS), F32),
        v((3, NW), BF16), v((128, 128), F32), v((128, 128), F32),
        v((BLOCKS, HEADS, 128, 128), F32), v((16, 8, 128), F32),
        v((4, 2, 128, 128), BF16), v((4, 2, 128, 128), BF16),
        v((4, 2, 128, 128), BF16), v((4, 2, 128, 128), BF16),
        v((3, 2, 128, 128), BF16), v((2, 128, 128), F32),
        v((BLOCKS, HEADS, 128, 128), F32), v((BLOCKS, HEADS, 128, 128), F32),
        v((128, 128), F32), v((128, 128), F32), v((ROWS, NW), BF16), v((HEADS, 128, 128), BF16),
        v((BLOCKS, HEADS, 128, 256), BF16), v((4, 8, 128), F32),
        dma((3,)), dma((5,)), dma((12,)), dma((4,)),
    ] + [dma((3,))] * 2 + [dma((15,))] * 2 + [dma((3,))] * 8 + [dma] * 8 + [pltpu.SemaphoreType.REGULAR]
    anywhere = pl.BlockSpec(memory_space=pltpu.HBM)
    return pl.pallas_call(
        kernel,
        out_shape=pltpu.VMEM((HALF, D), BF16),
        in_specs=[anywhere] * 14,
        out_specs=pl.BlockSpec(memory_space=pltpu.VMEM),
        scratch_shapes=scratch,
        compiler_params=pltpu.CompilerParams(
            collective_id=0, has_side_effects=True, vmem_limit_bytes=56 * 1024 * 1024
        ),
    )(
        tokens, norm_gain, log_decay, conv_taps, w_key, w_value, w_query,
        w_conv_in, w_conv_pre, w_conv_post, w_out_conv, w_out_ret,
        jnp.asarray(within), jnp.asarray(bases),
    )


def solution(mesh):
    in_specs = (
        P(("fs", "sp"), "tp"),
        P(),
        P(None, "tp"),
        P(None, "tp"),
        P(None, "tp"),
        P("tp", "sp"),
        P(None, "tp"),
        P(None, "tp"),
        P(None, "tp"),
        P(None, "tp"),
        P(),
        P(),
    )
    out_specs = P(("fs", "sp", "tp"), None)
    return jax.shard_map(body, mesh=mesh, in_specs=in_specs, out_specs=out_specs, check_vma=False)
```

```python
import functools

import jax
import jax.numpy as jnp
import numpy as np
from jax import lax
from jax.experimental import pallas as pl
from jax.experimental.pallas import tpu as pltpu
from jax.sharding import PartitionSpec as P

DH = 128
SPAN = 128
ROWS = 768
HALF = 384
BLOCKS = 6
HEADS = 4
KW = 1024
NW = 512
D = 2048
EPS = 1e-06
KEY_SCALE = 128.0 ** -0.5
F32 = jnp.float32
BF16 = jnp.bfloat16
MESH = pl.DeviceIdType.MESH
WEIGHTS = ("wk", "wv", "wq", "wci", "wcp", "wcq")


def rotation_tables(places):
    half = DH // 2
    rate = 10000.0 ** (-np.arange(half, dtype=np.float64) / half)
    inner = np.arange(SPAN, dtype=np.float64)[:, None] * rate[None, :]
    inner = np.concatenate([inner, inner], axis=1)
    sign = np.concatenate([-np.ones(half), np.ones(half)])[None, :]
    within = np.stack(
        [np.cos(inner), np.sin(inner), sign * np.cos(inner), sign * np.sin(inner)]
    ).astype(np.float32)
    start = np.arange(places * BLOCKS, dtype=np.float64) * SPAN
    outer = start[:, None] * rate[None, :]
    outer = np.concatenate([outer, outer], axis=1).reshape(places, BLOCKS, DH)
    bases = np.zeros((places, 16, DH), np.float32)
    bases[:, :BLOCKS] = np.cos(outer)
    bases[:, 8 : 8 + BLOCKS] = np.sin(outer)
    return within, bases


def mm(a, b):
    return jnp.dot(a, b, preferred_element_type=F32)


def kernel(
    tok, gain, ld, taps, wk, wv, wq, wci, wcp, wcq, woc, wor, tabs, bases,
    out,
    xo, go, gp, wbuf, wob, acc, kb, vb, qb, cib, postb, gbuf, cob, cor,
    retb, retr, inside, starts, oacc, ssb, pack, pack_far, rot_c, rot_s, key_c, key_s,
    tabv, basev, gainv, ldv, tapv, ldp, cumr, colrep, lall,
    a1, a2, b1, b2, bm, pre, fade, tails, cumc, endr, qs, entry, both, downv,
    sem_tok, sem_small, sem_w, sem_wo,
    ts, tr, ls, lr, a1s, a1r, a2s, a2r, b1s, b1r, b2s, b2r,
    hs, hr, cs, cr, rs, rr, ps, pr, met,
):
    sp = lax.axis_index("sp")
    tp = lax.axis_index("tp")
    x = lax.rem(sp, 4)
    z = lax.div(sp, 4)
    other = 1 - tp
    row_peer = [z * 4 + lax.rem(x + k, 4) for k in (1, 2, 3)]
    col_peer = [lax.rem(z + k, 4) * 4 + x for k in (1, 2, 3)]
    after = lax.rem(sp + 1, 16)
    ahead = [lax.rem(sp + k, 16) for k in range(1, 16)]
    behind = [lax.rem(sp + 16 - k, 16) for k in range(1, 16)]

    def remote(src, dst, send, recv, where):
        return pltpu.make_async_remote_copy(
            src_ref=src, dst_ref=dst, send_sem=send, recv_sem=recv,
            device_id=where, device_id_type=MESH,
        )

    own_k = pl.multiple_of(tp * KW, KW)
    far_k = pl.multiple_of(other * KW, KW)
    own_n = pl.multiple_of(tp * NW, NW)
    far_n = pl.multiple_of(other * NW, NW)
    own_rows = pl.ds(pl.multiple_of(tp * HALF, HALF), HALF)
    far_rows = pl.ds(pl.multiple_of(other * HALF, HALF), HALF)

    tok_load = [
        pltpu.make_async_copy(
            tok.at[pl.ds(c * 256, 256), :], xo.at[pl.ds(c * 256, 256), :], sem_tok.at[c]
        )
        for c in range(3)
    ]
    small = [
        pltpu.make_async_copy(ld, ldv, sem_small.at[0]),
        pltpu.make_async_copy(gain, gainv, sem_small.at[1]),
        pltpu.make_async_copy(taps, tapv, sem_small.at[2]),
        pltpu.make_async_copy(tabs, tabv, sem_small.at[3]),
        pltpu.make_async_copy(bases.at[sp], basev, sem_small.at[4]),
    ]
    hbm = dict(zip(WEIGHTS, (wk, wv, wq, wci, wcp, wcq)))
    index = {name: i for i, name in enumerate(WEIGHTS)}

    def w_load(name, part):
        i = index[name]
        rows = pl.ds(own_k if part == 0 else far_k, KW)
        return pltpu.make_async_copy(
            hbm[name].at[rows, :], wbuf.at[i, part], sem_w.at[i * 2 + part]
        )

    def wo_load(i, part):
        rows = pl.ds(own_n if part == 0 else far_n, NW)
        return pltpu.make_async_copy(
            (woc, wor)[i].at[rows, :], wob.at[i, part], sem_wo.at[i * 2 + part]
        )

    for copy in tok_load:
        copy.start()
    small[0].start()
    small[1].start()
    w_load("wk", 0).start()
    w_load("wv", 0).start()
    small[4].start()
    small[3].start()
    small[2].start()

    barrier = pltpu.get_barrier_semaphore()
    lall[...] = jnp.zeros_like(lall)
    a2[...] = jnp.zeros_like(a2)
    b1[...] = jnp.zeros_like(b1)
    a1[...] = jnp.zeros_like(a1)
    b2[...] = jnp.zeros_like(b2)

    @pl.when(tp == 0)
    def _():
        pl.semaphore_signal(barrier, inc=1, device_id={"tp": 1}, device_id_type=MESH)

    @pl.when(tp == 1)
    def _():
        pl.semaphore_wait(barrier, 1)
        pl.semaphore_signal(met, inc=1, device_id={"tp": 0}, device_id_type=MESH)

    @pl.when(tp == 0)
    def _():
        pl.semaphore_wait(met, 1)
        for peer in ahead:
            pl.semaphore_signal(barrier, inc=1, device_id={"sp": peer}, device_id_type=MESH)

    lane = lax.broadcasted_iota(jnp.int32, (SPAN, SPAN), 1)
    packed = jnp.zeros((SPAN, SPAN), F32)
    for i in range(BLOCKS):
        if i % 2 == 0:
            tok_load[i // 2].wait()
        rows = slice(i * 128, i * 128 + 128)
        value = xo[rows, :].astype(F32)
        squares = jnp.sum(value * value, axis=1, keepdims=True)
        spread = jnp.broadcast_to(squares, (SPAN, SPAN))
        ssb[rows, :] = spread
        packed = jnp.where(lane == i, spread, packed)
    pack[...] = packed

    pack_send = remote(pack, pack_far, ps, pr, {"tp": other})
    pack_send.start()
    ldp[...] = jnp.zeros_like(ldp)
    small[0].wait()
    for b in range(BLOCKS):
        ldp[b * 8 : b * 8 + HEADS, :] = ldv[:, b * SPAN : (b + 1) * SPAN]
    upper = (
        lax.broadcasted_iota(jnp.int32, (SPAN, SPAN), 0)
        <= lax.broadcasted_iota(jnp.int32, (SPAN, SPAN), 1)
    )
    ones = jnp.where(upper, 1.0, 0.0).astype(BF16)
    rest = ldp[...]
    total = jnp.zeros((SPAN, SPAN), F32)
    for _ in range(3):
        piece = rest.astype(BF16)
        total = total + mm(piece, ones)
        rest = rest - piece.astype(F32)
    cumr[...] = total
    cumc[...] = total.T
    ends = jnp.broadcast_to(total[:, SPAN - 1 : SPAN], (SPAN, SPAN))
    endr[...] = ends
    whole = ends[0:8]
    for b in range(1, BLOCKS):
        whole = whole + ends[b * 8 : b * 8 + 8]
    lall[sp] = whole

    def block_end(b, h):
        return endr[b * 8 + h : b * 8 + h + 1, :]

    def section(body):
        pl.when(sp < 16)(body)

    w_load("wq", 0).start()

    small[1].wait()
    weight = gainv[pl.ds(own_k, KW)].astype(F32).reshape(1, KW)
    pack_send.wait_recv()
    tok_send = [
        remote(
            go.at[pl.ds(c * 256, 256), :], gp.at[pl.ds(c * 256, 256), :],
            ts.at[c], tr.at[c], {"tp": other},
        )
        for c in range(3)
    ]
    for i in range(BLOCKS):
        rows = slice(i * 128, i * 128 + 128)
        level = ssb[rows, :] + jnp.broadcast_to(pack_far[:, i : i + 1], (SPAN, SPAN))
        scale = lax.rsqrt(level * (1.0 / D) + EPS)
        for c in range(KW // 128):
            at = slice(c * 128, c * 128 + 128)
            go[rows, at] = (xo[rows, at].astype(F32) * scale * weight[:, at]).astype(BF16)
        if i in (2, 4):
            tok_send[i // 2 - 1].start()
    tok_send[2].start()

    lower = (
        lax.broadcasted_iota(jnp.int32, (SPAN, SPAN), 0)
        >= lax.broadcasted_iota(jnp.int32, (SPAN, SPAN), 1)
    )

    def near_product(i):
        for n in range(2):
            cols = slice(n * 256, n * 256 + 256)
            acc[i, :, cols] = mm(go[...], wbuf[i, 0, :, cols])

    for name in ("wk", "wv", "wq"):
        w_load(name, 0).wait()
    for name in ("wk", "wv", "wq"):
        w_load(name, 1).start()
    for name in ("wci", "wcp"):
        for part in range(2):
            w_load(name, part).start()
    small[3].wait()
    small[4].wait()

    @section
    def _():
        near_product(0)
        for b in range(BLOCKS):
            rows = slice(b * 128, b * 128 + 128)
            base_c = basev[b : b + 1, :]
            base_s = basev[b + 8 : b + 9, :]
            rot_c[rows, :] = base_c * tabv[0] - base_s * tabv[1]
            rot_s[rows, :] = base_s * tabv[2] + base_c * tabv[3]
            key_c[rows, :] = rot_c[rows, :] * KEY_SCALE
            key_s[rows, :] = rot_s[rows, :] * KEY_SCALE
        near_product(1)
        for b in range(BLOCKS):
            for h in range(HEADS):
                i = b * 8 + h
                column = jnp.broadcast_to(cumc[:, i : i + 1], (SPAN, SPAN))
                colrep[b, h] = column
                gap = column - cumr[i : i + 1, :]
                fade[b, h] = jnp.where(lower, jnp.exp(jnp.minimum(gap, 0.0)), 0.0)
                tails[b, h] = jnp.exp(block_end(b, h) - column).astype(BF16)
        near_product(2)

    for copy in tok_send:
        copy.wait_recv()

    def rotated(value):
        return value * rot_c[...] + pltpu.roll(value, 64, axis=1) * rot_s[...]

    exchange = []

    def keys_of(n):
        cols = slice(n * 256, n * 256 + 256)
        kk = acc[0, :, cols] + mm(gp[...], wbuf[0, 1, :, cols])
        for j in range(2):
            at = slice(n * 256 + j * 128, n * 256 + j * 128 + 128)
            piece = kk[:, j * 128 : j * 128 + 128]
            kb[:, at] = (piece * key_c[...] + pltpu.roll(piece, 64, axis=1) * key_s[...]).astype(BF16)

    def values_of(n):
        cols = slice(n * 256, n * 256 + 256)
        vv = acc[1, :, cols] + mm(gp[...], wbuf[1, 1, :, cols])
        vb[:, cols] = vv.astype(BF16)

    def fresh_states(n):
        slot = a1.at[x] if n == 0 else b1.at[z]
        for j in range(2):
            h = n * 2 + j
            at = slice(h * 128, h * 128 + 128)
            whole = None
            for b in range(BLOCKS):
                rows = slice(b * 128, b * 128 + 128)
                weighted = vb[rows, at] * tails[b, h]
                fresh = lax.dot_general(
                    kb[rows, at], weighted, (((0,), (0,)), ((), ())),
                    preferred_element_type=F32,
                )
                if b == 0:
                    whole = fresh
                else:
                    starts[b, h] = whole.astype(BF16)
                    whole = jnp.exp(block_end(b, h)) * whole + fresh
            slot[j] = whole.astype(BF16)

    def start_along_row(copies, always):
        pl.when((x == 2) & always)(copies[1].start)
        for k in range(3):
            wanted = always | (x + k < 3)
            pl.when(wanted & (x != 2) if k == 1 else wanted)(copies[k].start)

    def send_states(n):
        for k in range(3):
            if n == 0:
                copy = remote(a1.at[x], a1.at[x], a1s.at[k], a1r.at[k], {"sp": row_peer[k]})
            else:
                copy = remote(b1.at[z], b1.at[z], b1s.at[k], b1r.at[k], {"sp": col_peer[k]})
            exchange.append(copy)
            if n == 1:
                pl.when(z + k < 3)(copy.start)
        if n == 0:
            start_along_row(exchange, z < 3)

    for name in ("wk", "wv", "wq"):
        w_load(name, 1).wait()
    @pl.when(tp == 0)
    def _():
        pl.semaphore_wait(barrier, 15)
        pl.semaphore_signal(met, inc=1, device_id={"tp": 1}, device_id_type=MESH)

    @pl.when(tp == 1)
    def _():
        pl.semaphore_wait(met, 1)

    def total_copy(k):
        return remote(lall.at[sp], lall.at[sp], ls.at[k], lr.at[k], {"sp": ahead[k]})

    for k in range(15):
        pl.when(lax.div(ahead[k], 4) >= z)(total_copy(k).start)

    @section
    def _():
        keys_of(0)
        keys_of(1)
        values_of(0)
        values_of(1)

    @section
    def _():
        fresh_states(0)
        fresh_states(1)

    send_states(0)
    send_states(1)

    for name in ("wci", "wcp"):
        for part in range(2):
            w_load(name, part).wait()
    for part in range(2):
        w_load("wcq", part).start()
    for i in range(2):
        for part in range(2):
            wo_load(i, part).start()

    def full_product(i, cols):
        return (
            mm(go[...], wbuf[i, 0, :, cols]) + mm(gp[...], wbuf[i, 1, :, cols])
        ).astype(BF16)

    @section
    def _():
        for n in range(2):
            cols = slice(n * 256, n * 256 + 256)
            cib[:, cols] = full_product(3, cols)
            gated = full_product(4, cols).astype(F32) * cib[:, cols].astype(F32)
            gated = gated.astype(BF16).astype(F32)
            for j in range(2):
                gbuf[n * 2 + j, 8 : 8 + ROWS, :] = gated[:, j * 128 : j * 128 + 128]

    halo = remote(
        gbuf.at[:, pl.ds(ROWS, 8), :], gbuf.at[:, pl.ds(0, 8), :], hs, hr, {"sp": after}
    )
    pl.when(sp < 15)(halo.start)

    for k in range(15):
        pl.when(lax.div(behind[k], 4) <= z)(total_copy(k).wait_recv)
    totals = [[lall[4 * i + j] for j in range(4)] for i in range(4)]
    line = [lall[4 * z + j] for j in range(4)]

    def between(low, high):
        parts = [
            jnp.where(jnp.logical_and(i > low, i < high), line[i], 0.0) for i in range(4)
        ]
        return (parts[0] + parts[1]) + (parts[2] + parts[3])

    row_sums = [(t[0] + t[1]) + (t[2] + t[3]) for t in totals]
    suffix = []
    for t in totals:
        parts = [jnp.where(j > x, t[j], 0.0) for j in range(4)]
        suffix.append((parts[0] + parts[1]) + (parts[2] + parts[3]))
    before_me = between(-1, x)

    def rows_between(low):
        parts = [
            jnp.where(jnp.logical_and(i > low, i < z), row_sums[i], 0.0) for i in range(4)
        ]
        return (parts[0] + parts[1]) + (parts[2] + parts[3])

    def lane_row(weight, h):
        return weight[h : h + 1, :]

    second = []
    above = [
        jnp.where(i < z, jnp.exp(suffix[i] + rows_between(i)), 0.0) for i in range(4)
    ]
    for k in range(3):
        pl.when(z > k)(exchange[3 + k].wait_recv)
    e_own = jnp.exp(before_me)
    for j in range(2):
        h = 2 + j
        column = lane_row(above[0], h) * b1[0, j].astype(F32)
        for i in range(1, 4):
            column = column + lane_row(above[i], h) * b1[i, j].astype(F32)
        mine = b1[z, j].astype(F32)
        b2[x, j] = (lane_row(e_own, h) * column).astype(BF16)
        for k in range(3):
            target = lax.rem(x + k + 1, 4)
            e_col = jnp.exp(between(-1, target))
            e_mine = jnp.where(x < target, jnp.exp(between(x, target)), 0.0)
            bm[k, j] = (lane_row(e_col, h) * column + lane_row(e_mine, h) * mine).astype(BF16)
    for k in range(3):
        copy = remote(bm.at[k], b2.at[x], b2s.at[k], b2r.at[k], {"sp": row_peer[k]})
        second.append(copy)
    start_along_row(second, z > 0)

    for part in range(2):
        w_load("wcq", part).wait()
    @section
    def _():
        for n in range(2):
            cols = slice(n * 256, n * 256 + 256)
            qq = acc[2, :, cols] + mm(gp[...], wbuf[2, 1, :, cols])
            for j in range(2):
                at = slice(n * 256 + j * 128, n * 256 + j * 128 + 128)
                qb[:, at] = rotated(qq[:, j * 128 : j * 128 + 128]).astype(BF16)
        postb[:, 0:256] = full_product(5, slice(0, 256))


    second += [
        remote(a2.at[z], a2.at[z], a2s.at[k], a2r.at[k], {"sp": col_peer[k]})
        for k in range(3)
    ]

    def pass_rows():
        to_end = [jnp.exp(between(i, 4)) for i in range(4)]
        to_me = [jnp.where(i < x, jnp.exp(between(i, x)), 0.0) for i in range(4)]
        for k in range(3):
            pl.when((z < 3) | (x > k))(exchange[k].wait_recv)
        for j in range(2):
            parts = [a1[i, j].astype(F32) for i in range(4)]
            row_state = lane_row(to_end[0], j) * parts[0]
            prefix = lane_row(to_me[0], j) * parts[0]
            for i in range(1, 4):
                row_state = row_state + lane_row(to_end[i], j) * parts[i]
                prefix = prefix + lane_row(to_me[i], j) * parts[i]
            pre[j] = prefix
            a2[z, j] = row_state.astype(BF16)
        for k in range(3):
            pl.when(z + k < 3)(second[3 + k].start)

    pass_rows()

    @section
    def _():
        postb[:, 256:512] = full_product(5, slice(256, 512))

    for i in range(4):
        downv[i] = jnp.where(i < z, jnp.exp(rows_between(i) + before_me), 0.0)

    small[2].wait()
    pl.when(sp > 0)(halo.wait_recv)

    @pl.when(sp == 0)
    def _():
        gbuf[:, 0:8, :] = jnp.zeros((4, 8, 128), F32)

    @section
    def _():
        for c in range(4):
            at = slice(c * 128, c * 128 + 128)
            summed = tapv[0:1, at].astype(F32) * gbuf[c, 6 : 6 + ROWS, :]
            for i in range(1, 3):
                summed = summed + tapv[i : i + 1, at].astype(F32) * gbuf[c, 6 + i : 6 + i + ROWS, :]
            cob[:, at] = (postb[:, at].astype(F32) * summed).astype(BF16)

    conv_send = remote(cob.at[far_rows, :], cor, cs, cr, {"tp": other})
    conv_send.start()

    for i in range(2):
        for part in range(2):
            wo_load(i, part).wait()

    def score_block(b):
        rows = slice(b * 128, b * 128 + 128)
        for h in range(HEADS):
            at = slice(h * 128, h * 128 + 128)
            scores = lax.dot_general(
                qb[rows, at], kb[rows, at], (((1,), (1,)), ((), ())),
                preferred_element_type=F32,
            )
            both[b, h, :, :128] = (scores * fade[b, h]).astype(BF16)
            query = qb[rows, at].astype(F32)
            if b == 0:
                qs[rows, at] = (query * jnp.exp(colrep[b, h])).astype(BF16)
            else:
                both[b, h, :, 128:] = (query * jnp.exp(colrep[b, h])).astype(BF16)
                offset = endr[h : h + 1, :]
                for e in range(1, b):
                    offset = offset + block_end(e, h)
                qs[rows, at] = (query * jnp.exp(colrep[b, h] + offset)).astype(BF16)

    def value_block(b):
        rows = slice(b * 128, b * 128 + 128)
        for h in range(HEADS):
            at = slice(h * 128, h * 128 + 128)
            if b == 0:
                inside[rows, at] = mm(both[b, h, :, :128], vb[rows, at])
            else:
                inside[rows, at] = mm(
                    both[b, h],
                    jnp.concatenate([vb[rows, at], starts[b, h]], axis=0),
                )

    @section
    def _():
        for n in range(8):
            cols = slice(n * 256, n * 256 + 256)
            oacc[:, cols] = mm(cob[own_rows, :], wob[0, 0, :, cols])
            if n < 6:
                score_block(n)
            if n >= 2:
                value_block(n - 2)

    conv_send.wait_recv()

    for k in range(15):
        pl.when(lax.div(ahead[k], 4) >= z)(total_copy(k).wait_send)
    for k in range(3):
        pl.when((z < 3) | (x + k < 3))(exchange[k].wait_send)
        pl.when(z + k < 3)(exchange[3 + k].wait_send)
    pl.when(sp < 15)(halo.wait_send)
    for copy in [pack_send] + tok_send:
        copy.wait_send()
    for k in range(3):
        pl.when((z > 0) | (x > k))(second[k].wait_recv)
        pl.when(z > k)(second[3 + k].wait_recv)
    down = [downv[i] for i in range(4)]
    for h in range(HEADS):
        j = h % 2
        if h < 2:
            state = pre[j]
            for i in range(4):
                state = state + lane_row(down[i], h) * a2[i, j].astype(F32)
        else:
            state = b2[0, j].astype(F32)
            for i in range(1, 4):
                state = state + b2[i, j].astype(F32)
        entry[h] = state.astype(BF16)

    def across(first, i):
        rows = pl.ds(pl.multiple_of(first + i * 128, 128), 128)
        for h in range(HEADS):
            at = slice(h * 128, h * 128 + 128)
            value = inside[rows, at] + mm(qs[rows, at], entry[h])
            level = jnp.mean(value * value, axis=1, keepdims=True)
            retb[rows, at] = (value * lax.rsqrt(level + EPS)).astype(BF16)

    @section
    def _():
        for i in range(3):
            across(other * HALF, i)

    ret_send = remote(retb.at[far_rows, :], retr, rs, rr, {"tp": other})
    ret_send.start()

    @section
    def _():
        for n in range(8):
            cols = slice(n * 256, n * 256 + 256)
            oacc[:, cols] += mm(cor[...], wob[0, 1, :, cols])
            if n < 3:
                across(tp * HALF, n)


    @section
    def _():
        for n in range(8):
            cols = slice(n * 256, n * 256 + 256)
            oacc[:, cols] += mm(retb[own_rows, :], wob[1, 0, :, cols])

    ret_send.wait_recv()

    @section
    def _():
        for n in range(8):
            cols = slice(n * 256, n * 256 + 256)
            out[:, cols] = (oacc[:, cols] + mm(retr[...], wob[1, 1, :, cols])).astype(BF16)

    for copy in [conv_send, ret_send]:
        copy.wait_send()
    for k in range(3):
        pl.when((z > 0) | (x + k < 3))(second[k].wait_send)
        pl.when(z + k < 3)(second[3 + k].wait_send)


def body(
    tokens, norm_gain, w_query, w_key, w_value, log_decay, w_conv_in, w_conv_pre,
    w_conv_post, conv_taps, w_out_ret, w_out_conv,
):
    within, bases = rotation_tables(16)
    dma = pltpu.SemaphoreType.DMA
    v = pltpu.VMEM
    scratch = [
        v((ROWS, KW), BF16), v((ROWS, KW), BF16), v((ROWS, KW), BF16),
        v((6, 2, KW, NW), BF16), v((2, 2, NW, D), BF16), v((3, ROWS, NW), F32),
        v((ROWS, NW), BF16), v((ROWS, NW), BF16), v((ROWS, NW), BF16),
        v((ROWS, NW), BF16), v((ROWS, NW), BF16), v((4, ROWS + 8, 128), F32),
        v((ROWS, NW), BF16), v((HALF, NW), BF16), v((ROWS, NW), BF16), v((HALF, NW), BF16),
        v((ROWS, NW), F32),
        v((BLOCKS, HEADS, 128, 128), BF16), v((HALF, D), F32),
        v((ROWS, 128), F32), v((128, 128), F32), v((128, 128), F32),
        v((ROWS, 128), F32), v((ROWS, 128), F32), v((ROWS, 128), F32), v((ROWS, 128), F32),
        v((4, 128, 128), F32), v((16, 128), F32), v((D,), BF16), v((HEADS, ROWS), F32),
        v((3, NW), BF16), v((128, 128), F32), v((128, 128), F32),
        v((BLOCKS, HEADS, 128, 128), F32), v((16, 8, 128), F32),
        v((4, 2, 128, 128), BF16), v((4, 2, 128, 128), BF16),
        v((4, 2, 128, 128), BF16), v((4, 2, 128, 128), BF16),
        v((3, 2, 128, 128), BF16), v((2, 128, 128), F32),
        v((BLOCKS, HEADS, 128, 128), F32), v((BLOCKS, HEADS, 128, 128), BF16),
        v((128, 128), F32), v((128, 128), F32), v((ROWS, NW), BF16), v((HEADS, 128, 128), BF16),
        v((BLOCKS, HEADS, 128, 256), BF16), v((4, 8, 128), F32),
        dma((3,)), dma((5,)), dma((12,)), dma((4,)),
    ] + [dma((3,))] * 2 + [dma((15,))] * 2 + [dma((3,))] * 8 + [dma] * 8 + [pltpu.SemaphoreType.REGULAR]
    anywhere = pl.BlockSpec(memory_space=pltpu.HBM)
    return pl.pallas_call(
        kernel,
        out_shape=pltpu.VMEM((HALF, D), BF16),
        in_specs=[anywhere] * 14,
        out_specs=pl.BlockSpec(memory_space=pltpu.VMEM),
        scratch_shapes=scratch,
        compiler_params=pltpu.CompilerParams(
            collective_id=0, has_side_effects=True, vmem_limit_bytes=56 * 1024 * 1024
        ),
    )(
        tokens, norm_gain, log_decay, conv_taps, w_key, w_value, w_query,
        w_conv_in, w_conv_pre, w_conv_post, w_out_conv, w_out_ret,
        jnp.asarray(within), jnp.asarray(bases),
    )


def solution(mesh):
    in_specs = (
        P(("fs", "sp"), "tp"),
        P(),
        P(None, "tp"),
        P(None, "tp"),
        P(None, "tp"),
        P("tp", "sp"),
        P(None, "tp"),
        P(None, "tp"),
        P(None, "tp"),
        P(None, "tp"),
        P(),
        P(),
    )
    out_specs = P(("fs", "sp", "tp"), None)
    return jax.shard_map(body, mesh=mesh, in_specs=in_specs, out_specs=out_specs, check_vma=False)
```

```python
import functools

import jax
import jax.numpy as jnp
import numpy as np
from jax import lax
from jax.experimental import pallas as pl
from jax.experimental.pallas import tpu as pltpu
from jax.sharding import PartitionSpec as P

DH = 128
SPAN = 128
ROWS = 768
HALF = 384
BLOCKS = 6
HEADS = 4
KW = 1024
NW = 512
D = 2048
EPS = 1e-06
KEY_SCALE = 128.0 ** -0.5
F32 = jnp.float32
BF16 = jnp.bfloat16
MESH = pl.DeviceIdType.MESH
WEIGHTS = ("wk", "wv", "wq", "wci", "wcp", "wcq")


def rotation_tables(places):
    half = DH // 2
    rate = 10000.0 ** (-np.arange(half, dtype=np.float64) / half)
    inner = np.arange(SPAN, dtype=np.float64)[:, None] * rate[None, :]
    inner = np.concatenate([inner, inner], axis=1)
    sign = np.concatenate([-np.ones(half), np.ones(half)])[None, :]
    within = np.stack(
        [np.cos(inner), np.sin(inner), sign * np.cos(inner), sign * np.sin(inner)]
    ).astype(np.float32)
    start = np.arange(places * BLOCKS, dtype=np.float64) * SPAN
    outer = start[:, None] * rate[None, :]
    outer = np.concatenate([outer, outer], axis=1).reshape(places, BLOCKS, DH)
    bases = np.zeros((places, 16, DH), np.float32)
    bases[:, :BLOCKS] = np.cos(outer)
    bases[:, 8 : 8 + BLOCKS] = np.sin(outer)
    return within, bases


def mm(a, b):
    return jnp.dot(a, b, preferred_element_type=F32)


def kernel(
    tok, gain, ld, taps, wk, wv, wq, wci, wcp, wcq, woc, wor, tabs, bases,
    out,
    xo, go, gp, wbuf, wob, acc, kb, vb, qb, cib, postb, gbuf, cob, cor,
    retb, retr, inside, starts, oacc, ssb, pack, pack_far, rot_c, rot_s, key_c, key_s,
    tabv, basev, gainv, ldv, tapv, ldp, cumr, colrep, lall,
    a1, a2, b1, b2, bm, pre, fade, tails, cumc, endr, qs, entry, both, downv,
    sem_tok, sem_small, sem_w, sem_wo,
    ts, tr, ls, lr, a1s, a1r, a2s, a2r, b1s, b1r, b2s, b2r,
    hs, hr, cs, cr, rs, rr, ps, pr, met,
):
    sp = lax.axis_index("sp")
    tp = lax.axis_index("tp")
    x = lax.rem(sp, 4)
    z = lax.div(sp, 4)
    other = 1 - tp
    row_peer = [z * 4 + lax.rem(x + k, 4) for k in (1, 2, 3)]
    col_peer = [lax.rem(z + k, 4) * 4 + x for k in (1, 2, 3)]
    after = lax.rem(sp + 1, 16)
    ahead = [lax.rem(sp + k, 16) for k in range(1, 16)]
    behind = [lax.rem(sp + 16 - k, 16) for k in range(1, 16)]

    def remote(src, dst, send, recv, where):
        return pltpu.make_async_remote_copy(
            src_ref=src, dst_ref=dst, send_sem=send, recv_sem=recv,
            device_id=where, device_id_type=MESH,
        )

    own_k = pl.multiple_of(tp * KW, KW)
    far_k = pl.multiple_of(other * KW, KW)
    own_n = pl.multiple_of(tp * NW, NW)
    far_n = pl.multiple_of(other * NW, NW)
    own_rows = pl.ds(pl.multiple_of(tp * HALF, HALF), HALF)
    far_rows = pl.ds(pl.multiple_of(other * HALF, HALF), HALF)

    tok_load = [
        pltpu.make_async_copy(
            tok.at[pl.ds(c * 256, 256), :], xo.at[pl.ds(c * 256, 256), :], sem_tok.at[c]
        )
        for c in range(3)
    ]
    small = [
        pltpu.make_async_copy(ld, ldv, sem_small.at[0]),
        pltpu.make_async_copy(gain, gainv, sem_small.at[1]),
        pltpu.make_async_copy(taps, tapv, sem_small.at[2]),
        pltpu.make_async_copy(tabs, tabv, sem_small.at[3]),
        pltpu.make_async_copy(bases.at[sp], basev, sem_small.at[4]),
    ]
    hbm = dict(zip(WEIGHTS, (wk, wv, wq, wci, wcp, wcq)))
    index = {name: i for i, name in enumerate(WEIGHTS)}

    def w_load(name, part):
        i = index[name]
        rows = pl.ds(own_k if part == 0 else far_k, KW)
        return pltpu.make_async_copy(
            hbm[name].at[rows, :], wbuf.at[i, part], sem_w.at[i * 2 + part]
        )

    def wo_load(i, part):
        rows = pl.ds(own_n if part == 0 else far_n, NW)
        return pltpu.make_async_copy(
            (woc, wor)[i].at[rows, :], wob.at[i, part], sem_wo.at[i * 2 + part]
        )

    for copy in tok_load:
        copy.start()
    small[0].start()
    small[1].start()
    w_load("wk", 0).start()
    w_load("wv", 0).start()
    small[4].start()
    small[3].start()
    small[2].start()

    barrier = pltpu.get_barrier_semaphore()
    lall[...] = jnp.zeros_like(lall)
    a2[...] = jnp.zeros_like(a2)
    b1[...] = jnp.zeros_like(b1)
    a1[...] = jnp.zeros_like(a1)
    b2[...] = jnp.zeros_like(b2)

    @pl.when(tp == 0)
    def _():
        pl.semaphore_signal(barrier, inc=1, device_id={"tp": 1}, device_id_type=MESH)

    @pl.when(tp == 1)
    def _():
        pl.semaphore_wait(barrier, 1)
        pl.semaphore_signal(met, inc=1, device_id={"tp": 0}, device_id_type=MESH)

    @pl.when(tp == 0)
    def _():
        pl.semaphore_wait(met, 1)
        for peer in ahead:
            pl.semaphore_signal(barrier, inc=1, device_id={"sp": peer}, device_id_type=MESH)

    lane = lax.broadcasted_iota(jnp.int32, (SPAN, SPAN), 1)
    packed = jnp.zeros((SPAN, SPAN), F32)
    for i in range(BLOCKS):
        if i % 2 == 0:
            tok_load[i // 2].wait()
        rows = slice(i * 128, i * 128 + 128)
        value = xo[rows, :].astype(F32)
        squares = jnp.sum(value * value, axis=1, keepdims=True)
        spread = jnp.broadcast_to(squares, (SPAN, SPAN))
        ssb[rows, :] = spread
        packed = jnp.where(lane == i, spread, packed)
    pack[...] = packed

    pack_send = remote(pack, pack_far, ps, pr, {"tp": other})
    pack_send.start()
    ldp[...] = jnp.zeros_like(ldp)
    small[0].wait()
    for b in range(BLOCKS):
        ldp[b * 8 : b * 8 + HEADS, :] = ldv[:, b * SPAN : (b + 1) * SPAN]
    upper = (
        lax.broadcasted_iota(jnp.int32, (SPAN, SPAN), 0)
        <= lax.broadcasted_iota(jnp.int32, (SPAN, SPAN), 1)
    )
    ones = jnp.where(upper, 1.0, 0.0).astype(BF16)
    rest = ldp[...]
    total = jnp.zeros((SPAN, SPAN), F32)
    for _ in range(3):
        piece = rest.astype(BF16)
        total = total + mm(piece, ones)
        rest = rest - piece.astype(F32)
    cumr[...] = total
    cumc[...] = total.T
    ends = jnp.broadcast_to(total[:, SPAN - 1 : SPAN], (SPAN, SPAN))
    endr[...] = ends
    whole = ends[0:8]
    for b in range(1, BLOCKS):
        whole = whole + ends[b * 8 : b * 8 + 8]
    lall[sp] = whole

    def block_end(b, h):
        return endr[b * 8 + h : b * 8 + h + 1, :]

    def section(body):
        pl.when(sp < 16)(body)

    w_load("wq", 0).start()

    small[1].wait()
    weight = gainv[pl.ds(own_k, KW)].astype(F32).reshape(1, KW)
    pack_send.wait_recv()
    tok_send = [
        remote(
            go.at[pl.ds(c * 256, 256), :], gp.at[pl.ds(c * 256, 256), :],
            ts.at[c], tr.at[c], {"tp": other},
        )
        for c in range(3)
    ]
    for i in range(BLOCKS):
        rows = slice(i * 128, i * 128 + 128)
        level = ssb[rows, :] + jnp.broadcast_to(pack_far[:, i : i + 1], (SPAN, SPAN))
        scale = lax.rsqrt(level * (1.0 / D) + EPS)
        for c in range(KW // 128):
            at = slice(c * 128, c * 128 + 128)
            go[rows, at] = (xo[rows, at].astype(F32) * scale * weight[:, at]).astype(BF16)
        if i in (2, 4):
            tok_send[i // 2 - 1].start()
    tok_send[2].start()

    lower = (
        lax.broadcasted_iota(jnp.int32, (SPAN, SPAN), 0)
        >= lax.broadcasted_iota(jnp.int32, (SPAN, SPAN), 1)
    )

    def near_product(i):
        for n in range(2):
            cols = slice(n * 256, n * 256 + 256)
            acc[i, :, cols] = mm(go[...], wbuf[i, 0, :, cols])

    for name in ("wk", "wv", "wq"):
        w_load(name, 0).wait()
    for name in ("wk", "wv", "wq"):
        w_load(name, 1).start()
    for name in ("wci", "wcp"):
        for part in range(2):
            w_load(name, part).start()
    small[3].wait()
    small[4].wait()

    @section
    def _():
        near_product(0)
        for b in range(BLOCKS):
            rows = slice(b * 128, b * 128 + 128)
            base_c = basev[b : b + 1, :]
            base_s = basev[b + 8 : b + 9, :]
            rot_c[rows, :] = base_c * tabv[0] - base_s * tabv[1]
            rot_s[rows, :] = base_s * tabv[2] + base_c * tabv[3]
            key_c[rows, :] = rot_c[rows, :] * KEY_SCALE
            key_s[rows, :] = rot_s[rows, :] * KEY_SCALE
        near_product(1)
        for b in range(BLOCKS):
            for h in range(HEADS):
                i = b * 8 + h
                column = jnp.broadcast_to(cumc[:, i : i + 1], (SPAN, SPAN))
                colrep[b, h] = column
                gap = column - cumr[i : i + 1, :]
                fade[b, h] = jnp.where(lower, jnp.exp(jnp.minimum(gap, 0.0)), 0.0)
                tails[b, h] = jnp.exp(block_end(b, h) - column).astype(BF16)
        near_product(2)

    for copy in tok_send:
        copy.wait_recv()

    def rotated(value):
        return value * rot_c[...] + pltpu.roll(value, 64, axis=1) * rot_s[...]

    exchange = [None] * 6

    def keys_of(n):
        cols = slice(n * 256, n * 256 + 256)
        kk = acc[0, :, cols] + mm(gp[...], wbuf[0, 1, :, cols])
        for j in range(2):
            at = slice(n * 256 + j * 128, n * 256 + j * 128 + 128)
            piece = kk[:, j * 128 : j * 128 + 128]
            kb[:, at] = (piece * key_c[...] + pltpu.roll(piece, 64, axis=1) * key_s[...]).astype(BF16)

    def values_of(n):
        cols = slice(n * 256, n * 256 + 256)
        vv = acc[1, :, cols] + mm(gp[...], wbuf[1, 1, :, cols])
        vb[:, cols] = vv.astype(BF16)

    def fresh_states(n):
        slot = a1.at[x] if n == 0 else b1.at[z]
        for j in range(2):
            h = n * 2 + j
            at = slice(h * 128, h * 128 + 128)
            whole = None
            for b in range(BLOCKS):
                rows = slice(b * 128, b * 128 + 128)
                weighted = vb[rows, at] * tails[b, h]
                fresh = lax.dot_general(
                    kb[rows, at], weighted, (((0,), (0,)), ((), ())),
                    preferred_element_type=F32,
                )
                if b == 0:
                    whole = fresh
                else:
                    starts[b, h] = whole.astype(BF16)
                    whole = jnp.exp(block_end(b, h)) * whole + fresh
            slot[j] = whole.astype(BF16)

    def start_along_row(copies, always):
        pl.when((x == 2) & always)(copies[1].start)
        for k in range(3):
            wanted = always | (x + k < 3)
            pl.when(wanted & (x != 2) if k == 1 else wanted)(copies[k].start)

    def send_states(n):
        for k in range(3):
            if n == 0:
                copy = remote(a1.at[x], a1.at[x], a1s.at[k], a1r.at[k], {"sp": row_peer[k]})
            else:
                copy = remote(b1.at[z], b1.at[z], b1s.at[k], b1r.at[k], {"sp": col_peer[k]})
            exchange[3 * n + k] = copy
            if n == 1:
                pl.when(z + k < 3)(copy.start)
        if n == 0:
            start_along_row(exchange, z < 3)

    for name in ("wk", "wv", "wq"):
        w_load(name, 1).wait()
    @pl.when(tp == 0)
    def _():
        pl.semaphore_wait(barrier, 15)
        pl.semaphore_signal(met, inc=1, device_id={"tp": 1}, device_id_type=MESH)

    @pl.when(tp == 1)
    def _():
        pl.semaphore_wait(met, 1)

    def total_copy(k):
        return remote(lall.at[sp], lall.at[sp], ls, lr, {"sp": ahead[k]})

    def all_totals(count):
        part = lall.at[pl.ds(0, count)]
        return remote(part, part, ls, lr, {"sp": ahead[0]})

    for k in range(15):
        pl.when(lax.div(ahead[k], 4) >= z)(total_copy(k).start)

    @section
    def _():
        keys_of(0)
        keys_of(1)
        values_of(0)
        values_of(1)

    @section
    def _():
        fresh_states(0)
        fresh_states(1)

    send_states(1)
    send_states(0)

    for name in ("wci", "wcp"):
        for part in range(2):
            w_load(name, part).wait()
    for part in range(2):
        w_load("wcq", part).start()
    for i in range(2):
        for part in range(2):
            wo_load(i, part).start()

    def full_product(i, cols):
        return (
            mm(go[...], wbuf[i, 0, :, cols]) + mm(gp[...], wbuf[i, 1, :, cols])
        ).astype(BF16)

    @section
    def _():
        for n in range(2):
            cols = slice(n * 256, n * 256 + 256)
            cib[:, cols] = full_product(3, cols)
            gated = full_product(4, cols).astype(F32) * cib[:, cols].astype(F32)
            gated = gated.astype(BF16).astype(F32)
            for j in range(2):
                gbuf[n * 2 + j, 8 : 8 + ROWS, :] = gated[:, j * 128 : j * 128 + 128]

    halo = remote(
        gbuf.at[:, pl.ds(ROWS, 8), :], gbuf.at[:, pl.ds(0, 8), :], hs, hr, {"sp": after}
    )
    pl.when(sp < 15)(halo.start)

    for i in range(4):
        pl.when(z == i)(all_totals(4 * i + 3).wait_recv)
    totals = [[lall[4 * i + j] for j in range(4)] for i in range(4)]
    line = [lall[4 * z + j] for j in range(4)]

    def between(low, high):
        parts = [
            jnp.where(jnp.logical_and(i > low, i < high), line[i], 0.0) for i in range(4)
        ]
        return (parts[0] + parts[1]) + (parts[2] + parts[3])

    row_sums = [(t[0] + t[1]) + (t[2] + t[3]) for t in totals]
    suffix = []
    for t in totals:
        parts = [jnp.where(j > x, t[j], 0.0) for j in range(4)]
        suffix.append((parts[0] + parts[1]) + (parts[2] + parts[3]))
    before_me = between(-1, x)

    def rows_between(low):
        parts = [
            jnp.where(jnp.logical_and(i > low, i < z), row_sums[i], 0.0) for i in range(4)
        ]
        return (parts[0] + parts[1]) + (parts[2] + parts[3])

    def lane_row(weight, h):
        return weight[h : h + 1, :]

    second = []
    above = [
        jnp.where(i < z, jnp.exp(suffix[i] + rows_between(i)), 0.0) for i in range(4)
    ]
    for k in range(3):
        pl.when(z > k)(exchange[3 + k].wait_recv)
    e_own = jnp.exp(before_me)
    for j in range(2):
        h = 2 + j
        column = lane_row(above[0], h) * b1[0, j].astype(F32)
        for i in range(1, 4):
            column = column + lane_row(above[i], h) * b1[i, j].astype(F32)
        mine = b1[z, j].astype(F32)
        b2[x, j] = (lane_row(e_own, h) * column).astype(BF16)
        for k in range(3):
            target = lax.rem(x + k + 1, 4)
            e_col = jnp.exp(between(-1, target))
            e_mine = jnp.where(x < target, jnp.exp(between(x, target)), 0.0)
            bm[k, j] = (lane_row(e_col, h) * column + lane_row(e_mine, h) * mine).astype(BF16)
    for k in range(3):
        copy = remote(bm.at[k], b2.at[x], b2s.at[k], b2r.at[k], {"sp": row_peer[k]})
        second.append(copy)
    start_along_row(second, z > 0)

    for part in range(2):
        w_load("wcq", part).wait()
    @section
    def _():
        for n in range(2):
            cols = slice(n * 256, n * 256 + 256)
            qq = acc[2, :, cols] + mm(gp[...], wbuf[2, 1, :, cols])
            for j in range(2):
                at = slice(n * 256 + j * 128, n * 256 + j * 128 + 128)
                qb[:, at] = rotated(qq[:, j * 128 : j * 128 + 128]).astype(BF16)
        postb[:, 0:256] = full_product(5, slice(0, 256))


    second += [
        remote(a2.at[z], a2.at[z], a2s.at[k], a2r.at[k], {"sp": col_peer[k]})
        for k in range(3)
    ]

    def pass_rows():
        to_end = [jnp.exp(between(i, 4)) for i in range(4)]
        to_me = [jnp.where(i < x, jnp.exp(between(i, x)), 0.0) for i in range(4)]
        for k in range(3):
            pl.when((z < 3) | (x > k))(exchange[k].wait_recv)
        for j in range(2):
            parts = [a1[i, j].astype(F32) for i in range(4)]
            row_state = lane_row(to_end[0], j) * parts[0]
            prefix = lane_row(to_me[0], j) * parts[0]
            for i in range(1, 4):
                row_state = row_state + lane_row(to_end[i], j) * parts[i]
                prefix = prefix + lane_row(to_me[i], j) * parts[i]
            pre[j] = prefix
            a2[z, j] = row_state.astype(BF16)
        for k in range(3):
            pl.when(z + k < 3)(second[3 + k].start)

    pass_rows()

    @section
    def _():
        postb[:, 256:512] = full_product(5, slice(256, 512))

    for i in range(4):
        downv[i] = jnp.where(i < z, jnp.exp(rows_between(i) + before_me), 0.0)

    small[2].wait()
    pl.when(sp > 0)(halo.wait_recv)

    @pl.when(sp == 0)
    def _():
        gbuf[:, 0:8, :] = jnp.zeros((4, 8, 128), F32)

    @section
    def _():
        for c in range(4):
            at = slice(c * 128, c * 128 + 128)
            summed = tapv[0:1, at].astype(F32) * gbuf[c, 6 : 6 + ROWS, :]
            for i in range(1, 3):
                summed = summed + tapv[i : i + 1, at].astype(F32) * gbuf[c, 6 + i : 6 + i + ROWS, :]
            cob[:, at] = (postb[:, at].astype(F32) * summed).astype(BF16)

    conv_send = remote(cob.at[far_rows, :], cor, cs, cr, {"tp": other})
    conv_send.start()

    for i in range(2):
        for part in range(2):
            wo_load(i, part).wait()

    def score_block(b):
        rows = slice(b * 128, b * 128 + 128)
        for h in range(HEADS):
            at = slice(h * 128, h * 128 + 128)
            scores = lax.dot_general(
                qb[rows, at], kb[rows, at], (((1,), (1,)), ((), ())),
                preferred_element_type=F32,
            )
            both[b, h, :, :128] = (scores * fade[b, h]).astype(BF16)
            query = qb[rows, at].astype(F32)
            if b == 0:
                qs[rows, at] = (query * jnp.exp(colrep[b, h])).astype(BF16)
            else:
                both[b, h, :, 128:] = (query * jnp.exp(colrep[b, h])).astype(BF16)
                offset = endr[h : h + 1, :]
                for e in range(1, b):
                    offset = offset + block_end(e, h)
                qs[rows, at] = (query * jnp.exp(colrep[b, h] + offset)).astype(BF16)

    def value_block(b):
        rows = slice(b * 128, b * 128 + 128)
        for h in range(HEADS):
            at = slice(h * 128, h * 128 + 128)
            if b == 0:
                inside[rows, at] = mm(both[b, h, :, :128], vb[rows, at])
            else:
                inside[rows, at] = mm(
                    both[b, h],
                    jnp.concatenate([vb[rows, at], starts[b, h]], axis=0),
                )

    @section
    def _():
        for n in range(8):
            cols = slice(n * 256, n * 256 + 256)
            oacc[:, cols] = mm(cob[own_rows, :], wob[0, 0, :, cols])
            if n < 6:
                score_block(n)
            if n >= 2:
                value_block(n - 2)

    conv_send.wait_recv()

    for i in range(4):
        pl.when(z == i)(all_totals(15 - 4 * i).wait_send)
    for k in range(3):
        pl.when((z < 3) | (x + k < 3))(exchange[k].wait_send)
        pl.when(z + k < 3)(exchange[3 + k].wait_send)
    pl.when(sp < 15)(halo.wait_send)
    for copy in [pack_send] + tok_send:
        copy.wait_send()
    for k in range(3):
        pl.when((z > 0) | (x > k))(second[k].wait_recv)
        pl.when(z > k)(second[3 + k].wait_recv)
    down = [downv[i] for i in range(4)]
    for h in range(HEADS):
        j = h % 2
        if h < 2:
            state = pre[j]
            for i in range(4):
                state = state + lane_row(down[i], h) * a2[i, j].astype(F32)
        else:
            state = b2[0, j].astype(F32)
            for i in range(1, 4):
                state = state + b2[i, j].astype(F32)
        entry[h] = state.astype(BF16)

    def across(first, i):
        rows = pl.ds(pl.multiple_of(first + i * 128, 128), 128)
        for h in range(HEADS):
            at = slice(h * 128, h * 128 + 128)
            value = inside[rows, at] + mm(qs[rows, at], entry[h])
            level = jnp.mean(value * value, axis=1, keepdims=True)
            retb[rows, at] = (value * lax.rsqrt(level + EPS)).astype(BF16)

    @section
    def _():
        for i in range(3):
            across(other * HALF, i)

    ret_send = remote(retb.at[far_rows, :], retr, rs, rr, {"tp": other})
    ret_send.start()

    @section
    def _():
        for n in range(8):
            cols = slice(n * 256, n * 256 + 256)
            oacc[:, cols] += mm(cor[...], wob[0, 1, :, cols])
            if n < 3:
                across(tp * HALF, n)


    @section
    def _():
        for n in range(8):
            cols = slice(n * 256, n * 256 + 256)
            oacc[:, cols] += mm(retb[own_rows, :], wob[1, 0, :, cols])

    ret_send.wait_recv()

    @section
    def _():
        for n in range(8):
            cols = slice(n * 256, n * 256 + 256)
            out[:, cols] = (oacc[:, cols] + mm(retr[...], wob[1, 1, :, cols])).astype(BF16)

    for copy in [conv_send, ret_send]:
        copy.wait_send()
    for k in range(3):
        pl.when((z > 0) | (x + k < 3))(second[k].wait_send)
        pl.when(z + k < 3)(second[3 + k].wait_send)


def body(
    tokens, norm_gain, w_query, w_key, w_value, log_decay, w_conv_in, w_conv_pre,
    w_conv_post, conv_taps, w_out_ret, w_out_conv,
):
    within, bases = rotation_tables(16)
    dma = pltpu.SemaphoreType.DMA
    v = pltpu.VMEM
    scratch = [
        v((ROWS, KW), BF16), v((ROWS, KW), BF16), v((ROWS, KW), BF16),
        v((6, 2, KW, NW), BF16), v((2, 2, NW, D), BF16), v((3, ROWS, NW), F32),
        v((ROWS, NW), BF16), v((ROWS, NW), BF16), v((ROWS, NW), BF16),
        v((ROWS, NW), BF16), v((ROWS, NW), BF16), v((4, ROWS + 8, 128), F32),
        v((ROWS, NW), BF16), v((HALF, NW), BF16), v((ROWS, NW), BF16), v((HALF, NW), BF16),
        v((ROWS, NW), F32),
        v((BLOCKS, HEADS, 128, 128), BF16), v((HALF, D), F32),
        v((ROWS, 128), F32), v((128, 128), F32), v((128, 128), F32),
        v((ROWS, 128), F32), v((ROWS, 128), F32), v((ROWS, 128), F32), v((ROWS, 128), F32),
        v((4, 128, 128), F32), v((16, 128), F32), v((D,), BF16), v((HEADS, ROWS), F32),
        v((3, NW), BF16), v((128, 128), F32), v((128, 128), F32),
        v((BLOCKS, HEADS, 128, 128), F32), v((16, 8, 128), F32),
        v((4, 2, 128, 128), BF16), v((4, 2, 128, 128), BF16),
        v((4, 2, 128, 128), BF16), v((4, 2, 128, 128), BF16),
        v((3, 2, 128, 128), BF16), v((2, 128, 128), F32),
        v((BLOCKS, HEADS, 128, 128), F32), v((BLOCKS, HEADS, 128, 128), BF16),
        v((128, 128), F32), v((128, 128), F32), v((ROWS, NW), BF16), v((HEADS, 128, 128), BF16),
        v((BLOCKS, HEADS, 128, 256), BF16), v((4, 8, 128), F32),
        dma((3,)), dma((5,)), dma((12,)), dma((4,)),
    ] + [dma((3,))] * 2 + [dma] * 2 + [dma((3,))] * 8 + [dma] * 8 + [pltpu.SemaphoreType.REGULAR]
    anywhere = pl.BlockSpec(memory_space=pltpu.HBM)
    return pl.pallas_call(
        kernel,
        out_shape=pltpu.VMEM((HALF, D), BF16),
        in_specs=[anywhere] * 14,
        out_specs=pl.BlockSpec(memory_space=pltpu.VMEM),
        scratch_shapes=scratch,
        compiler_params=pltpu.CompilerParams(
            collective_id=0, has_side_effects=True, vmem_limit_bytes=56 * 1024 * 1024
        ),
    )(
        tokens, norm_gain, log_decay, conv_taps, w_key, w_value, w_query,
        w_conv_in, w_conv_pre, w_conv_post, w_out_conv, w_out_ret,
        jnp.asarray(within), jnp.asarray(bases),
    )


def solution(mesh):
    in_specs = (
        P(("fs", "sp"), "tp"),
        P(),
        P(None, "tp"),
        P(None, "tp"),
        P(None, "tp"),
        P("tp", "sp"),
        P(None, "tp"),
        P(None, "tp"),
        P(None, "tp"),
        P(None, "tp"),
        P(),
        P(),
    )
    out_specs = P(("fs", "sp", "tp"), None)
    return jax.shard_map(body, mesh=mesh, in_specs=in_specs, out_specs=out_specs, check_vma=False)
```
